512 devices in a mesh: gr: 2 (over z_hi), sp: 32 (over z_lo, y), tp: 8 (over x, core).
Axes of the slice: x: 4, y: 4, z: 16 (z_hi: 2, z_lo: 8; z = z_hi * 8 + z_lo), core: 2. Of those that a mesh axis runs over, the one named last changes fastest.
Arguments:
- prompt: bfloat16 [2, 8192, 4096], P('gr', 'sp', 'tp'), parts along dimension 0, may hold values from -6 to 6
- key_weight: bfloat16 [4096, 4096], P(None, 'tp'), may hold values from -0.09375 to 0.09375
- value_weight: bfloat16 [4096, 4096], P(None, 'tp'), may hold values from -0.375 to 0.375
- beta_weight: bfloat16 [4096, 32], P(None, 'tp'), may hold values from -0.09375 to 0.09375
- beta_bias: float32 [32], P('tp'), may hold values from -4.5 to -0.5
- decay_rate: float32 [32], P('tp'), may hold values from 0.1 to 3
- new_query: bfloat16 [2, 32, 128], P('gr', 'tp'), parts along dimension 0, may hold values from -6 to 6
- read_gain: float32 [128], replicated, may hold values from 0.1 to 1.9
Outputs:
- state_cache: bfloat16 [2, 32, 128, 128], P('gr', 'tp', 'sp'), parts along dimension 0
- first_read: float32 [2, 32, 128], P('gr', 'tp'), parts along dimension 0
The draws below stay inside these ranges and needn't reach their ends.
There are 2 independent parts, one for each index of `gr`. The reference program is written for one: setup_inputs(seed, part) draws one part's arguments, and reference() takes and returns one part's arrays. A program takes and returns all parts, laid end to end along the dimension named above; an argument that names none is the same for every part. Nothing has to cross between parts.
All inputs are finite; a program needn't handle non-finite values.
Results may differ from the reference program's by a relative error of at most 0.013.
Values may be sent and summed in bfloat16 or wider, within the bound.
No kernel may reach another device: no remote copies, remote signals or barrier semaphores. Data moves between devices by JAX's collectives and lax.ppermute only.
A program may use at most 64 MiB of HBM per device.

```python
import math
import jax
import jax.numpy as jnp
from jax import lax

D = 4096
HEADS = 32
HDIM = 128
BLOCK = 64
LEN = 8192


def draw_prompt(key, part):
    shared_key = jax.random.fold_in(key, 11)
    single_key = jax.random.fold_in(key, 12)
    run_count = LEN // BLOCK
    common = 1.5 * jax.random.normal(shared_key, (run_count, 1, D), jnp.float32)
    own_part = 0.75 * jax.random.normal(single_key, (run_count, BLOCK, D), jnp.float32)
    combined = jnp.clip(common + own_part, -6.0, 6.0).reshape(1, LEN, D)
    return combined.astype(jnp.bfloat16)


def level_of(key, extent, split, least, high):
    def one(position, blocks):
        draws = jax.random.uniform(jax.random.fold_in(jax.random.fold_in(key, 6), position), (blocks,), jnp.float32, least / len(split), high / len(split))
        return jnp.repeat(jnp.exp(draws), extent[position] // blocks).reshape((-1,) + (1,) * (len(extent) - position - 1))

    factor_of = one(*split[0])
    for cut in split[1:]:
        factor_of = factor_of * one(*cut)
    return factor_of


def gaussian(own_key, dims, spread, most, split=(), held_as=jnp.bfloat16):
    result = jax.random.normal(own_key, dims, jnp.float32) * spread
    if len(split) > 0:
        result = level_of(own_key, dims, split, -0.22, 0.18) * result
    return jnp.clip(result, min=-most, max=most).astype(held_as)


def setup_inputs(seed: int = 0, part: int = 0) -> dict:
    arg_keys = jax.random.split(jax.random.key(seed), 9)
    own_keys = jax.random.split(jax.random.fold_in(arg_keys[8], part), 9)
    prompt = draw_prompt(jax.random.fold_in(jax.random.fold_in(arg_keys[8], part), 71), part)
    key_weight = gaussian(arg_keys[1], (D, HEADS * HDIM), D ** -0.5, 0.09375, ((1, 8),))
    value_weight = gaussian(arg_keys[2], (D, HEADS * HDIM), (D // 16) ** -0.5, 0.375, ((1, 8),))
    beta_weight = gaussian(arg_keys[3], (D, HEADS), D ** -0.5, 0.09375, ((1, 8),))
    beta_bias = jnp.clip(-4.5 + 4.0 * jax.random.uniform(arg_keys[4], (HEADS,), jnp.float32) ** level_of(arg_keys[4], (HEADS,), ((0, 8),), -0.2, 0.2), -4.5, -0.5)
    decay_rate = jnp.clip(jnp.exp(math.log(3.0) - 3.4011974 * jax.random.uniform(arg_keys[5], (HEADS,), jnp.float32) ** level_of(arg_keys[5], (HEADS,), ((0, 8),), -0.2, 0.2)), 0.1, 3.0)
    new_query = gaussian(own_keys[6], (1, HEADS, HDIM), 1.0, 6.0, ((1, 8),))
    read_gain = jnp.clip(1.0 + 0.18 * jax.random.normal(arg_keys[7], (HDIM,), jnp.float32), 0.1, 1.9)
    return dict(prompt=prompt, key_weight=key_weight, value_weight=value_weight, beta_weight=beta_weight, beta_bias=beta_bias, decay_rate=decay_rate, new_query=new_query, read_gain=read_gain)


def reference(prompt, key_weight, value_weight, beta_weight, beta_bias, decay_rate, new_query, read_gain):
    tokens = prompt[0]
    key_proj = jnp.dot(tokens, key_weight, preferred_element_type=jnp.float32).astype(jnp.bfloat16)
    value_proj = jnp.dot(tokens, value_weight, preferred_element_type=jnp.float32).astype(jnp.bfloat16)
    beta_pre = jnp.dot(tokens, beta_weight, preferred_element_type=jnp.float32)
    key_proj = lax.optimization_barrier(key_proj)
    value_proj = lax.optimization_barrier(value_proj)
    key_rows = key_proj.astype(jnp.float32).reshape(LEN, HEADS, HDIM)
    key_rows = key_rows * lax.rsqrt(lax.optimization_barrier(jnp.sum(key_rows * key_rows, axis=-1, keepdims=True)) + 1.0)
    values = value_proj.astype(jnp.float32).reshape(LEN, HEADS, HDIM)
    strength = jax.nn.sigmoid(beta_pre + beta_bias)
    retain = jnp.exp(-decay_rate / LEN)

    def advance(memory_matrix, inputs):
        single_key_row, value_row, beta_row = inputs
        retrieved_values = jnp.einsum('jg,jgb->jb', single_key_row, memory_matrix, precision=lax.Precision.HIGHEST)
        written_update = beta_row[:, None, None] * single_key_row[:, :, None]
        memory_matrix = retain[:, None, None] * (memory_matrix - written_update * retrieved_values[:, None, :])
        memory_matrix = memory_matrix + written_update * value_row[:, None, :]
        return (memory_matrix, None)
    initial = jnp.zeros((HEADS, HDIM, HDIM), jnp.float32)
    closing_state = lax.scan(advance, initial, (key_rows, values, strength))[0]
    normalized_query = new_query[0].astype(jnp.float32)
    normalized_query = normalized_query * lax.rsqrt(lax.optimization_barrier(jnp.sum(normalized_query * normalized_query, axis=-1, keepdims=True)) + 1.0)
    unscaled_read = jnp.einsum('jg,jgb->jb', normalized_query, closing_state, precision=lax.Precision.HIGHEST)
    read_out = unscaled_read * lax.rsqrt(lax.optimization_barrier(jnp.mean(unscaled_read * unscaled_read, axis=-1, keepdims=True)) + 0.05) * read_gain
    return (closing_state.astype(jnp.bfloat16)[None], read_out[None])
```

```python
import functools

import jax
import jax.numpy as jnp
from jax import lax
from jax.experimental import pallas as pl
from jax.experimental.pallas import tpu as pltpu
from jax.sharding import Mesh
from jax.sharding import PartitionSpec as P

SPAN = 128
F32, BF16 = jnp.float32, jnp.bfloat16
NT = (((1,), (1,)), ((), ()))
NN = (((1,), (0,)), ((), ()))
TN = (((0,), (0,)), ((), ()))


def dot(a, b, dims=NN):
    return lax.dot_general(a.astype(BF16), b.astype(BF16), dims, preferred_element_type=F32)


def halves(a):
    high = a.astype(BF16)
    return high, (a - high.astype(F32)).astype(BF16)


def span_kernel(
    full_len, core_ref, xa_ref, xb_ref, kw_ref, vw_ref, bw_ref, bias_ref, rate_ref, out_ref
):
    core = core_ref[0]
    seg_len = xa_ref.shape[1]
    heads = out_ref.shape[0]
    wide = 256
    pieces = []
    for j in range(xa_ref.shape[0]):
        pieces.append((xa_ref, j, 2 * j + core))
        pieces.append((xb_ref, j, 2 * j + 1 - core))

    def projected(weight_ref, n):
        total = None
        for ref, j, place in pieces:
            part = dot(ref[j], weight_ref[place, :, n * wide : (n + 1) * wide])
            total = part if total is None else total + part
        return total

    beta = None
    for ref, j, place in pieces:
        part = dot(ref[j], bw_ref[place], NT)
        beta = part if beta is None else beta + part
    beta = jax.nn.sigmoid(beta[:, :heads] + bias_ref[...])
    keys = [projected(kw_ref, n).astype(BF16) for n in range(heads * SPAN // wide)]
    values = [projected(vw_ref, n).astype(BF16) for n in range(heads * SPAN // wide)]

    row = lax.broadcasted_iota(jnp.int32, (SPAN, SPAN), 0)
    col = lax.broadcasted_iota(jnp.int32, (SPAN, SPAN), 1)
    apart = row ^ col
    lower = row > col
    eye = (row == col).astype(F32)
    place = lax.broadcasted_iota(jnp.int32, (1, SPAN), 1)
    later = (SPAN - 1 - place).astype(F32)

    jobs = [(h, s) for h in range(heads) for s in range(seg_len // SPAN)]
    per = wide // SPAN
    kp, vp, low, inv, scale_col, key_row, val_row, decay = ([] for _ in range(8))
    for h, s in jobs:
        k = keys[h // per][s * SPAN : (s + 1) * SPAN, (h % per) * SPAN : (h % per + 1) * SPAN]
        v = values[h // per][s * SPAN : (s + 1) * SPAN, (h % per) * SPAN : (h % per + 1) * SPAN]
        gram = dot(k, k, NT)
        diag = gram * eye
        s_col = lax.rsqrt(jnp.sum(diag, axis=1, keepdims=True) + 1.0)
        s_row = lax.rsqrt(jnp.sum(diag, axis=0, keepdims=True) + 1.0)
        b_col = beta[s * SPAN : (s + 1) * SPAN, h : h + 1]
        b_row = jnp.sum(eye * b_col, axis=0, keepdims=True)
        log_step = -rate_ref[0, h] / full_len
        lo = jnp.where(lower, gram * (b_col * s_col) * s_row, 0.0)
        kp.append(k)
        vp.append(v)
        low.append(lo)
        inv.append(eye - jnp.where(apart == 1, lo, 0.0))
        scale_col.append(s_col)
        key_row.append(b_row * s_row)
        val_row.append(b_row * jnp.exp(log_step * later))
        decay.append(jnp.exp(jnp.zeros((1, SPAN), F32) + log_step * SPAN))

    level = 1
    while 2 ** level < SPAN:
        mask = (apart >> level) == 1
        low_m = [jnp.where(mask, lo, 0.0).astype(BF16) for lo in low]
        inv_b = [t.astype(BF16) for t in inv]
        mid = [dot(m, t) for m, t in zip(low_m, inv_b)]
        fix = [dot(t, m) for t, m in zip(inv_b, mid)]
        inv = [t - f for t, f in zip(inv, fix)]
        level += 1

    for i in range(len(jobs)):
        low_h, low_l = halves(low[i])
        inv_h, inv_l = halves(inv[i])
        left = eye - inv[i] - (dot(low_h, inv_h) + (dot(low_h, inv_l) + dot(low_l, inv_h)))
        inv[i] = inv[i] + dot(inv_h, left)

    made = []
    for i in range(len(jobs)):
        tk_h, tk_l = halves(inv[i] * key_row[i])
        tv_h, tv_l = halves(inv[i] * val_row[i])
        x_key = dot(tk_h, kp[i]) + dot(tk_l, kp[i])
        x_val = dot(tv_h, vp[i]) + dot(tv_l, vp[i])
        x_h, x_l = halves(
            scale_col[i] * jnp.concatenate([-x_key * decay[i], x_val], axis=1)
        )
        both = dot(kp[i], x_h, TN) + dot(kp[i], x_l, TN)
        made.append((both[:, :SPAN] + eye * (decay[i] - 1.0), both[:, SPAN:]))

    for h in range(heads):
        total = None
        for s in range(seg_len // SPAN):
            change, write = made[h * (seg_len // SPAN) + s]
            now = jnp.concatenate([change, write], axis=1)
            total = now if total is None else now + total + dot(change, total)
        out_ref[h] = total.astype(BF16)


def joined(parts):
    total = parts[0].astype(F32)
    for j in range(1, parts.shape[0]):
        now = parts[j]
        total = total + now.astype(F32) + dot(now[:, :SPAN], total)
    return total


def to_all(value, axis):
    copies = jnp.broadcast_to(value[None], (lax.axis_size(axis), *value.shape))
    return lax.all_to_all(copies, axis, 0, 0, tiled=True)


def swapped(value, axis):
    return lax.ppermute(value, axis, [(0, 1), (1, 0)])


def shards(
    prompt, key_weight, value_weight, beta_weight, beta_bias, decay_rate, new_query, read_gain
):
    seg_len, part = prompt.shape[1], prompt.shape[2]
    heads = beta_weight.shape[1]
    tp = lax.axis_size(("x", "c"))
    sp = lax.axis_size(("zh", "zq", "y"))
    full_len = seg_len * sp
    core = lax.axis_index("c")
    mine = to_all(prompt[0], "x")
    other = swapped(mine, "c")
    vmem = pl.BlockSpec(memory_space=pltpu.VMEM)
    smem = pl.BlockSpec(memory_space=pltpu.SMEM)
    span = pl.pallas_call(
        functools.partial(span_kernel, full_len),
        out_shape=jax.ShapeDtypeStruct((heads, SPAN, 2 * SPAN), BF16),
        in_specs=[smem] + [vmem] * 6 + [smem],
        out_specs=vmem,
        compiler_params=pltpu.CompilerParams(vmem_limit_bytes=40 * 1024 * 1024),
        name="span",
    )(
        core.astype(jnp.int32)[None],
        mine,
        other,
        key_weight.reshape(tp, part, -1),
        value_weight.reshape(tp, part, -1),
        jnp.transpose(beta_weight.reshape(tp, part, heads), (0, 2, 1)),
        beta_bias[None],
        decay_rate[None],
    )
    by_head = lax.all_to_all(span, "y", 0, 0, tiled=True)
    level_y = joined(by_head).astype(BF16)
    level_z = joined(to_all(level_y, "zq")).astype(BF16)

    upper = lax.axis_index("zh") == 1
    y = lax.axis_index("y")
    own_z = lax.axis_index("zh") * lax.axis_size("zq") + lax.axis_index("zq")
    partner_z = own_z ^ lax.axis_size("zq")
    rows = SPAN // (2 * lax.axis_size("zq"))
    query = lax.dynamic_index_in_dim(new_query[0], y, 0, keepdims=True).astype(F32)
    query = query * lax.rsqrt(jnp.sum(query * query, axis=-1, keepdims=True) + 1.0)
    pulled = dot(query, level_z) + 0.0

    def block_for(z):
        picked = lax.dynamic_slice_in_dim(level_z, z * rows, rows, 0)
        tail = jnp.zeros((SPAN // 2 - rows - 1, 2 * SPAN), BF16)
        return jnp.concatenate([picked, pulled.astype(BF16), tail], axis=0)

    send_rows = block_for(partner_z).reshape(SPAN, SPAN)
    sent = jnp.where(upper, send_rows, level_z[:, SPAN:])
    came = swapped(sent, "zh")
    late = jnp.where(upper, block_for(own_z), came.reshape(SPAN // 2, 2 * SPAN))
    early = jnp.where(upper, came, level_z[:, SPAN:])
    q_high, q_low = halves(query)
    kept = jnp.concatenate(
        [
            lax.dynamic_slice_in_dim(early, own_z * rows, rows, 0).astype(F32),
            dot(q_high, early) + dot(q_low, early),
        ],
        axis=0,
    )
    final = dot(late[: rows + 1, :SPAN], early) + late[: rows + 1, SPAN:].astype(F32) + kept
    each = rows // lax.axis_size("y")
    read = jnp.broadcast_to(final[None, rows:], (lax.axis_size("y"), 1, SPAN))
    packed = jnp.concatenate([final[:rows].reshape(-1, each, SPAN), read], axis=1)
    home = lax.all_to_all(packed, "y", 0, 0, tiled=True)
    raw = home[:, each]
    read_out = raw * lax.rsqrt(jnp.mean(raw * raw, axis=-1, keepdims=True) + 0.05) * read_gain
    return (home[:, :each].astype(BF16)[None], read_out[None])


def solution(mesh):
    y, x = 4, 4
    zq = 4
    zh = mesh.shape["sp"] // (zq * y)
    finer = Mesh(
        mesh.devices.reshape(mesh.shape["gr"], zh, zq, y, x, mesh.shape["tp"] // x),
        ("gr", "zh", "zq", "y", "x", "c"),
    )
    sp, tp = ("zh", "zq", "y"), ("x", "c")
    return jax.shard_map(
        shards,
        mesh=finer,
        in_specs=(
            P("gr", sp, tp),
            P(None, tp),
            P(None, tp),
            P(None, tp),
            P(tp),
            P(tp),
            P("gr", tp, None),
            P(),
        ),
        out_specs=(P("gr", tp, sp, None), P("gr", tp, None)),
        check_vma=False,
    )
```

```python
import functools

import jax
import jax.numpy as jnp
from jax import lax
from jax.experimental import pallas as pl
from jax.experimental.pallas import tpu as pltpu
from jax.sharding import Mesh
from jax.sharding import PartitionSpec as P

SPAN = 128
WIDE = 256
F32, BF16 = jnp.float32, jnp.bfloat16
NT = (((1,), (1,)), ((), ()))
NN = (((1,), (0,)), ((), ()))
TN = (((0,), (0,)), ((), ()))


def dot(a, b, dims=NN):
    return lax.dot_general(a.astype(BF16), b.astype(BF16), dims, preferred_element_type=F32)


def halves(a):
    high = a.astype(BF16)
    return high, (a - high.astype(F32)).astype(BF16)


def beta_sum(x_ref, aux_ref, side):
    count, _, part = x_ref.shape
    total = None
    for j in range(count):
        start = pl.multiple_of((2 * j + side) * part, part)
        now = dot(x_ref[j], aux_ref[:, pl.ds(start, part)], NT)
        total = now if total is None else total + now
    return total


def first_kernel(
    core_ref, x_ref, aux_ref, kw_ref, vw_ref, acc_ref, beta_ref, kw_out, vw_out,
    kw_own, vw_own, own_sem, other_sem,
):
    core = core_ref[0]
    count = x_ref.shape[0]
    cols = kw_ref.shape[2]

    def copy(src, dst, sem):
        made = pltpu.make_async_copy(src, dst, sem)
        made.start()
        return made

    key_copies = [copy(kw_ref.at[2 * j + core], kw_own.at[j], own_sem.at[0, j]) for j in range(count)]
    value_copies = [copy(vw_ref.at[2 * j + core], vw_own.at[j], own_sem.at[1, j]) for j in range(count)]
    others = []
    for j in range(count):
        others.append(copy(kw_ref.at[2 * j + 1 - core], kw_out.at[j], other_sem.at[0, j]))
        others.append(copy(vw_ref.at[2 * j + 1 - core], vw_out.at[j], other_sem.at[1, j]))
    for done in key_copies:
        done.wait()
    for n in range(0, cols, WIDE):
        total = None
        for j in range(count):
            part = dot(x_ref[j], kw_own[j, :, n : n + WIDE])
            total = part if total is None else total + part
        acc_ref[:, n : n + WIDE] = total
    beta_ref[...] = beta_sum(x_ref, aux_ref, core)
    for done in value_copies:
        done.wait()
    for n in range(0, cols, WIDE):
        total = None
        for j in range(count):
            part = dot(x_ref[j], vw_own[j, :, n : n + WIDE])
            total = part if total is None else total + part
        acc_ref[:, cols + n : cols + n + WIDE] = total
    for done in others:
        done.wait()


def span_kernel(
    full_len, core_ref, x_ref, aux_ref, acc_ref, beta_ref, kw_ref, vw_ref, out_ref,
):
    core = core_ref[0]
    count, seg_len = x_ref.shape[:2]
    heads = out_ref.shape[0]
    cols = kw_ref.shape[2]

    def projected(weight_ref, n, start):
        total = acc_ref[:, start + n : start + n + WIDE]
        for j in range(count):
            total = total + dot(x_ref[j], weight_ref[j, :, n : n + WIDE])
        return total.astype(BF16)

    all_feat = 2 * count * x_ref.shape[2]
    tail_h = aux_ref[:, all_feat : all_feat + SPAN]
    lane = lax.broadcasted_iota(jnp.int32, tail_h.shape, 1)
    sub = lax.broadcasted_iota(jnp.int32, tail_h.shape, 0)
    bias = jnp.sum(jnp.where(lane == sub, tail_h, 0.0), axis=0, keepdims=True)[:, :heads]
    beta = beta_ref[...] + beta_sum(x_ref, aux_ref, 1 - core)
    beta = jax.nn.sigmoid(beta + bias)
    keys = [projected(kw_ref, n, 0) for n in range(0, cols, WIDE)]
    values = [projected(vw_ref, n, cols) for n in range(0, cols, WIDE)]

    row = lax.broadcasted_iota(jnp.int32, (SPAN, SPAN), 0)
    col = lax.broadcasted_iota(jnp.int32, (SPAN, SPAN), 1)
    apart = row ^ col
    lower = row > col
    eye = (row == col).astype(F32)
    place = lax.broadcasted_iota(jnp.int32, (1, SPAN), 1)
    later = (SPAN - 1 - place).astype(F32)

    jobs = [(h, s) for h in range(heads) for s in range(seg_len // SPAN)]
    per = WIDE // SPAN
    kp, vp, low, inv, scale_col, key_row, val_row, decay = ([] for _ in range(8))
    for h, s in jobs:
        k = keys[h // per][s * SPAN : (s + 1) * SPAN, (h % per) * SPAN : (h % per + 1) * SPAN]
        v = values[h // per][s * SPAN : (s + 1) * SPAN, (h % per) * SPAN : (h % per + 1) * SPAN]
        gram = dot(k, k, NT)
        diag = gram * eye
        s_col = lax.rsqrt(jnp.sum(diag, axis=1, keepdims=True) + 1.0)
        s_row = lax.rsqrt(jnp.sum(diag, axis=0, keepdims=True) + 1.0)
        b_col = beta[s * SPAN : (s + 1) * SPAN, h : h + 1]
        b_row = jnp.sum(eye * b_col, axis=0, keepdims=True)
        log_step = -aux_ref[h : h + 1, all_feat + SPAN : all_feat + SPAN + 1] / full_len
        lo = jnp.where(lower, gram * (b_col * s_col) * s_row, 0.0)
        kp.append(k)
        vp.append(v)
        low.append(lo)
        inv.append(eye - jnp.where(apart == 1, lo, 0.0))
        scale_col.append(s_col)
        key_row.append(b_row * s_row)
        val_row.append(b_row * jnp.exp(log_step * later))
        decay.append(jnp.exp(log_step * SPAN + jnp.zeros((1, SPAN), F32)))

    level = 1
    while 2 ** level < SPAN:
        mask = (apart >> level) == 1
        low_m = [jnp.where(mask, lo, 0.0).astype(BF16) for lo in low]
        inv_b = [t.astype(BF16) for t in inv]
        mid = [dot(m, t) for m, t in zip(low_m, inv_b)]
        fix = [dot(t, m) for t, m in zip(inv_b, mid)]
        inv = [t - f for t, f in zip(inv, fix)]
        level += 1

    for i in range(len(jobs)):
        low_h, low_l = halves(low[i])
        inv_h, inv_l = halves(inv[i])
        both_l = jnp.concatenate([low_h, low_l], axis=1)
        left = eye - inv[i] - (dot(both_l, jnp.concatenate([inv_h, inv_h], axis=0)) + dot(low_h, inv_l))
        inv[i] = inv[i] + dot(inv_h, left)

    made = []
    for i in range(len(jobs)):
        twice = jnp.concatenate([kp[i], kp[i]], axis=0)
        x_key = dot(jnp.concatenate(halves(inv[i] * key_row[i]), axis=1), twice)
        x_val = dot(
            jnp.concatenate(halves(inv[i] * val_row[i]), axis=1),
            jnp.concatenate([vp[i], vp[i]], axis=0),
        )
        solved = scale_col[i] * jnp.concatenate([-x_key * decay[i], x_val], axis=1)
        both = dot(twice, jnp.concatenate(halves(solved), axis=0), TN)
        made.append((both[:, :SPAN] + eye * (decay[i] - 1.0), both[:, SPAN:]))

    for h in range(heads):
        total = None
        for s in range(seg_len // SPAN):
            change, write = made[h * (seg_len // SPAN) + s]
            now = jnp.concatenate([change, write], axis=1)
            total = now if total is None else now + total + dot(change, total)
        out_ref[h] = total.astype(BF16)


def joined(parts):
    total = parts[0].astype(F32)
    for j in range(1, parts.shape[0]):
        now = parts[j]
        total = total + now.astype(F32) + dot(now[:, :SPAN], total)
    return total


def to_all(value, axis):
    copies = jnp.broadcast_to(value[None], (lax.axis_size(axis), *value.shape))
    return lax.all_to_all(copies, axis, 0, 0, tiled=True)


def swapped(value, axis):
    return lax.ppermute(value, axis, [(0, 1), (1, 0)])


def shards(
    prompt, key_weight, value_weight, beta_weight, beta_bias, decay_rate, new_query, read_gain
):
    seg_len, part = prompt.shape[1], prompt.shape[2]
    heads = beta_weight.shape[1]
    tp = lax.axis_size(("x", "c"))
    sp = lax.axis_size(("zh", "zq", "y"))
    full_len = seg_len * sp
    core = lax.axis_index("c")
    mine = to_all(prompt[0], "x")
    other = swapped(mine, "c")
    vmem = pl.BlockSpec(memory_space=pltpu.VMEM)
    smem = pl.BlockSpec(memory_space=pltpu.SMEM)
    hbm = pl.BlockSpec(memory_space=pltpu.HBM)
    sides, cols = mine.shape[0], key_weight.shape[1]
    core_of = core.astype(jnp.int32)[None]
    kept_weight = jax.ShapeDtypeStruct((sides, part, cols), BF16)
    aux = jnp.concatenate(
        [
            jnp.transpose(beta_weight).astype(F32),
            jnp.broadcast_to(beta_bias[:, None], (heads, SPAN)),
            jnp.broadcast_to(decay_rate[:, None], (heads, SPAN)),
        ],
        axis=1,
    )
    acc, beta, key_rest, value_rest = pl.pallas_call(
        first_kernel,
        out_shape=(
            jax.ShapeDtypeStruct((seg_len, 2 * cols), F32),
            jax.ShapeDtypeStruct((seg_len, heads), F32),
            kept_weight,
            kept_weight,
        ),
        in_specs=[smem, vmem, vmem, hbm, hbm],
        out_specs=[vmem] * 4,
        scratch_shapes=[
            pltpu.VMEM((sides, part, cols), BF16),
            pltpu.VMEM((sides, part, cols), BF16),
            pltpu.SemaphoreType.DMA((2, sides)),
            pltpu.SemaphoreType.DMA((2, sides)),
        ],
        compiler_params=pltpu.CompilerParams(vmem_limit_bytes=45 * 1024 * 1024),
        cost_estimate=pl.CostEstimate(
            flops=4 * seg_len * sides * part * cols,
            bytes_accessed=1,
            transcendentals=0,
        ),
        name="first",
    )(
        core_of,
        mine,
        aux,
        key_weight.reshape(tp, part, cols),
        value_weight.reshape(tp, part, cols),
    )
    span = pl.pallas_call(
        functools.partial(span_kernel, full_len),
        out_shape=jax.ShapeDtypeStruct((heads, SPAN, 2 * SPAN), BF16),
        in_specs=[smem] + [vmem] * 6,
        out_specs=vmem,
        compiler_params=pltpu.CompilerParams(vmem_limit_bytes=32 * 1024 * 1024),
        name="span",
    )(core_of, other, aux, acc, beta, key_rest, value_rest)
    by_head = lax.all_to_all(span, "y", 0, 0, tiled=True)
    level_y = joined(by_head).astype(BF16)
    level_z = joined(to_all(level_y, "zq")).astype(BF16)

    upper = lax.axis_index("zh") == 1
    y = lax.axis_index("y")
    own_z = lax.axis_index("zh") * lax.axis_size("zq") + lax.axis_index("zq")
    partner_z = own_z ^ lax.axis_size("zq")
    rows = SPAN // (2 * lax.axis_size("zq"))
    query = lax.dynamic_index_in_dim(new_query[0], y, 0, keepdims=True).astype(F32)
    query = query * lax.rsqrt(jnp.sum(query * query, axis=-1, keepdims=True) + 1.0)
    pulled = dot(query, level_z) + 0.0

    def block_for(z):
        picked = lax.dynamic_slice_in_dim(level_z, z * rows, rows, 0)
        tail = jnp.zeros((SPAN // 2 - rows - 1, 2 * SPAN), BF16)
        return jnp.concatenate([picked, pulled.astype(BF16), tail], axis=0)

    send_rows = block_for(partner_z).reshape(SPAN, SPAN)
    sent = jnp.where(upper, send_rows, level_z[:, SPAN:])
    came = swapped(sent, "zh")
    late = jnp.where(upper, block_for(own_z), came.reshape(SPAN // 2, 2 * SPAN))
    early = jnp.where(upper, came, level_z[:, SPAN:])
    q_high, q_low = halves(query)
    kept = jnp.concatenate(
        [
            lax.dynamic_slice_in_dim(early, own_z * rows, rows, 0).astype(F32),
            dot(q_high, early) + dot(q_low, early),
        ],
        axis=0,
    )
    final = dot(late[: rows + 1, :SPAN], early) + late[: rows + 1, SPAN:].astype(F32) + kept
    each = rows // lax.axis_size("y")
    read = jnp.broadcast_to(final[None, rows:], (lax.axis_size("y"), 1, SPAN))
    packed = jnp.concatenate([final[:rows].reshape(-1, each, SPAN), read], axis=1)
    home = lax.all_to_all(packed, "y", 0, 0, tiled=True)
    raw = home[:, each]
    read_out = raw * lax.rsqrt(jnp.mean(raw * raw, axis=-1, keepdims=True) + 0.05) * read_gain
    return (home[:, :each].astype(BF16)[None], read_out[None])


def solution(mesh):
    y, x = 4, 4
    zq = 4
    zh = mesh.shape["sp"] // (zq * y)
    finer = Mesh(
        mesh.devices.reshape(mesh.shape["gr"], zh, zq, y, x, mesh.shape["tp"] // x),
        ("gr", "zh", "zq", "y", "x", "c"),
    )
    sp, tp = ("zh", "zq", "y"), ("x", "c")
    return jax.shard_map(
        shards,
        mesh=finer,
        in_specs=(
            P("gr", sp, tp),
            P(None, tp),
            P(None, tp),
            P(None, tp),
            P(tp),
            P(tp),
            P("gr", tp, None),
            P(),
        ),
        out_specs=(P("gr", tp, sp, None), P("gr", tp, None)),
        check_vma=False,
    )
```

```python
import functools

import jax
import jax.numpy as jnp
from jax import lax
from jax.experimental import pallas as pl
from jax.experimental.pallas import tpu as pltpu
from jax.sharding import Mesh
from jax.sharding import PartitionSpec as P

SPAN = 128
WIDE = 256
FIRST_MIB = 47
SPAN_MIB = 48
F32, BF16 = jnp.float32, jnp.bfloat16
NT = (((1,), (1,)), ((), ()))
NN = (((1,), (0,)), ((), ()))
TN = (((0,), (0,)), ((), ()))


def dot(a, b, dims=NN):
    return lax.dot_general(a.astype(BF16), b.astype(BF16), dims, preferred_element_type=F32)


def halves(a):
    high = a.astype(BF16)
    return high, (a - high.astype(F32)).astype(BF16)


def beta_sum(x_ref, aux_ref, side, heads):
    count, _, part = x_ref.shape
    total = None
    for j in range(count):
        start = pl.multiple_of((2 * j + side) * part, part)
        now = dot(x_ref[j], aux_ref[0:heads, pl.ds(start, part)], NT)
        total = now if total is None else total + now
    return total


def project(x_ref, weight_ref, place, add_ref, out_ref, start):
    count = x_ref.shape[0]

    def tile(n, carry):
        here = pl.ds(pl.multiple_of(n * WIDE, WIDE), WIDE)
        there = pl.ds(pl.multiple_of(n * WIDE + start, WIDE), WIDE)
        total = None if add_ref is None else add_ref[:, there]
        for j in range(count):
            part = dot(x_ref[j], weight_ref[place(j), :, here])
            total = part if total is None else total + part
        out_ref[:, there] = total.astype(out_ref.dtype)
        return carry

    lax.fori_loop(0, weight_ref.shape[2] // WIDE, tile, 0)


def copied(src, dst, sem):
    made = pltpu.make_async_copy(src, dst, sem)
    made.start()
    return made


def first_kernel(
    x_ref, aux_ref, kw_ref, vw_ref, acc_ref, beta_ref, kw_out, kw_own, vw_own, sems,
):
    core = lax.axis_index("c")
    sides = range(x_ref.shape[0])
    cols = kw_ref.shape[2]
    keys = [copied(kw_ref.at[2 * j + core], kw_own.at[j], sems.at[0, j]) for j in sides]
    values = [copied(vw_ref.at[2 * j + core], vw_own.at[j], sems.at[1, j]) for j in sides]
    others = [copied(kw_ref.at[2 * j + 1 - core], kw_out.at[j], sems.at[2, j]) for j in sides]
    beta_ref[...] = beta_sum(x_ref, aux_ref, core, beta_ref.shape[1])
    for done in keys:
        done.wait()
    project(x_ref, kw_own, lambda j: j, None, acc_ref, 0)
    for done in values:
        done.wait()
    project(x_ref, vw_own, lambda j: j, None, acc_ref, cols)
    for done in others:
        done.wait()


def odd_rows(value, size):
    return jnp.concatenate(
        [value[r : r + size] for r in range(size, SPAN, 2 * size)], axis=0
    )


def woven(even, odd, size):
    parts = []
    for i in range(SPAN // (2 * size)):
        r = 2 * size * i
        parts.append(
            jnp.zeros((size, SPAN), F32) if even is None else even[r : r + size]
        )
        parts.append(odd[size * i : size * (i + 1)])
    return jnp.concatenate(parts, axis=0)


def span_kernel(
    full_len, x_ref, aux_ref, acc_ref, beta_ref, kw_ref, vw_ref, out_ref, vw_rest, sems,
):
    core = lax.axis_index("c")
    count, seg_len = x_ref.shape[:2]
    heads = out_ref.shape[0]
    cols = kw_ref.shape[2]
    rest = [
        copied(vw_ref.at[2 * j + 1 - core], vw_rest.at[j], sems.at[j]) for j in range(count)
    ]
    bias = aux_ref[heads : heads + 1, 0:heads]
    beta = beta_ref[...] + beta_sum(x_ref, aux_ref, 1 - core, heads)
    beta = jax.nn.sigmoid(beta + bias)
    keys = []
    for n in range(0, cols, WIDE):
        total = acc_ref[:, n : n + WIDE]
        for j in range(count):
            total = total + dot(x_ref[j], kw_ref[j, :, n : n + WIDE])
        keys.append(total.astype(BF16))

    row = lax.broadcasted_iota(jnp.int32, (SPAN, SPAN), 0)
    col = lax.broadcasted_iota(jnp.int32, (SPAN, SPAN), 1)
    apart = row ^ col
    lower = row > col
    eye = (row == col).astype(F32)
    place = lax.broadcasted_iota(jnp.int32, (1, SPAN), 1)
    later = (SPAN - 1 - place).astype(F32)

    jobs = [(h, s) for h in range(heads) for s in range(seg_len // SPAN)]
    per = WIDE // SPAN

    def cut(tiles, h, s):
        return tiles[h // per][s * SPAN : (s + 1) * SPAN, (h % per) * SPAN : (h % per + 1) * SPAN]

    low, inv, scale_col, key_row, val_row, decay = ([] for _ in range(6))
    for h, s in jobs:
        k = cut(keys, h, s)
        gram = dot(k, k, NT)
        diag = gram * eye
        s_col = lax.rsqrt(jnp.sum(diag, axis=1, keepdims=True) + 1.0)
        s_row = lax.rsqrt(jnp.sum(diag, axis=0, keepdims=True) + 1.0)
        b_col = beta[s * SPAN : (s + 1) * SPAN, h : h + 1]
        b_row = jnp.sum(eye * b_col, axis=0, keepdims=True)
        log_step = -aux_ref[heads + 1 : heads + 2, h : h + 1] / full_len
        lo = jnp.where(lower, gram * (b_col * s_col) * s_row, 0.0)
        low.append(lo)
        inv.append(eye - jnp.where(apart == 1, lo, 0.0))
        scale_col.append(s_col)
        key_row.append(b_row * s_row)
        val_row.append(b_row * jnp.exp(log_step * later))
        decay.append(jnp.exp(log_step * SPAN + jnp.zeros((1, SPAN), F32)))

    for done in rest:
        done.wait()
    pending = [(n, j) for n in range(0, cols, WIDE) for j in range(count)]
    value_acc = {n: acc_ref[:, cols + n : cols + n + WIDE] for n in range(0, cols, WIDE)}
    levels = SPAN.bit_length() - 2

    for level in range(1, levels + 1):
        size = 2**level
        inv_b = [t.astype(BF16) for t in inv]
        if size < 8:
            mask = (apart >> level) == 1
            low_m = [jnp.where(mask, lo, 0.0) for lo in low]
            mid = [dot(m, t) for m, t in zip(low_m, inv_b)]
            inv = [t - dot(tb, m) for t, tb, m in zip(inv, inv_b, mid)]
        else:
            mask = (odd_rows(apart, size) >> level) == 1
            low_m = [jnp.where(mask, odd_rows(lo, size), 0.0) for lo in low]
            mid = [woven(None, dot(m, t), size) for m, t in zip(low_m, inv_b)]
            inv = [
                woven(t, odd_rows(t, size) - dot(odd_rows(t, size), m), size)
                for t, m in zip(inv, mid)
            ]
        for _ in range(-(-len(pending) // (levels + 1 - level))):
            n, j = pending.pop(0)
            value_acc[n] = value_acc[n] + dot(x_ref[j], vw_rest[j, :, n : n + WIDE])
    values = [value_acc[n].astype(BF16) for n in range(0, cols, WIDE)]

    for i in range(len(jobs)):
        low_h, low_l = halves(low[i])
        inv_h, inv_l = halves(inv[i])
        both_l = jnp.concatenate([low_h, low_l], axis=1)
        twice = jnp.concatenate([inv_h, inv_h], axis=0)
        left = eye - inv[i] - (dot(both_l, twice) + dot(low_h, inv_l))
        inv[i] = inv[i] + dot(inv_h, left)

    made = []
    for i, (h, s) in enumerate(jobs):
        k, v = cut(keys, h, s), cut(values, h, s)
        twice = jnp.concatenate([k, k], axis=0)
        x_key = dot(jnp.concatenate(halves(inv[i] * key_row[i]), axis=1), twice)
        x_val = dot(
            jnp.concatenate(halves(inv[i] * val_row[i]), axis=1),
            jnp.concatenate([v, v], axis=0),
        )
        solved = scale_col[i] * jnp.concatenate([-x_key * decay[i], x_val], axis=1)
        both = dot(twice, jnp.concatenate(halves(solved), axis=0), TN)
        made.append((both[:, :SPAN] + eye * (decay[i] - 1.0), both[:, SPAN:]))

    for h in range(heads):
        total = None
        for s in range(seg_len // SPAN):
            change, write = made[h * (seg_len // SPAN) + s]
            now = jnp.concatenate([change, write], axis=1)
            total = now if total is None else now + total + dot(change, total)
        out_ref[h] = total.astype(BF16)


def joined(parts):
    total = parts[0].astype(F32)
    for j in range(1, parts.shape[0]):
        now = parts[j]
        total = total + now.astype(F32) + dot(now[:, :SPAN], total)
    return total


def to_all(value, axis):
    copies = jnp.broadcast_to(value[None], (lax.axis_size(axis), *value.shape))
    return lax.all_to_all(copies, axis, 0, 0, tiled=True)


def swapped(value, axis):
    return lax.ppermute(value, axis, [(0, 1), (1, 0)])


def shards(
    prompt, key_weight, value_weight, beta_weight, beta_bias, decay_rate, new_query, read_gain
):
    seg_len, part = prompt.shape[1], prompt.shape[2]
    heads = beta_weight.shape[1]
    tp = lax.axis_size(("x", "c"))
    sp = lax.axis_size(("zh", "zq", "y"))
    full_len = seg_len * sp
    mine = to_all(prompt[0], "x")
    other = swapped(mine, "c")
    vmem = pl.BlockSpec(memory_space=pltpu.VMEM)
    hbm = pl.BlockSpec(memory_space=pltpu.HBM)
    sides, cols = mine.shape[0], key_weight.shape[1]
    feat = tp * part
    aux = (
        jnp.pad(jnp.transpose(beta_weight).astype(F32), ((0, heads), (0, 0)))
        + jnp.pad(beta_bias[None], ((heads, heads - 1), (0, feat - heads)))
        + jnp.pad(decay_rate[None], ((heads + 1, heads - 2), (0, feat - heads)))
    )
    key_near = key_weight.reshape(tp, part, cols)
    value_near = value_weight.reshape(tp, part, cols)
    kept = pltpu.VMEM((sides, part, cols), BF16)
    acc, beta, key_rest = pl.pallas_call(
        first_kernel,
        out_shape=(
            jax.ShapeDtypeStruct((seg_len, 2 * cols), F32),
            jax.ShapeDtypeStruct((seg_len, heads), F32),
            jax.ShapeDtypeStruct((sides, part, cols), BF16),
        ),
        in_specs=[vmem, vmem, hbm, hbm],
        out_specs=[vmem] * 3,
        scratch_shapes=[kept, kept, pltpu.SemaphoreType.DMA((3, sides))],
        compiler_params=pltpu.CompilerParams(vmem_limit_bytes=FIRST_MIB * 1024 * 1024),
        cost_estimate=pl.CostEstimate(
            flops=4 * seg_len * sides * part * cols, bytes_accessed=1, transcendentals=0
        ),
        name="first",
    )(mine, aux, key_near, value_near)
    span = pl.pallas_call(
        functools.partial(span_kernel, full_len),
        out_shape=jax.ShapeDtypeStruct((heads, SPAN, 2 * SPAN), BF16),
        in_specs=[vmem] * 5 + [hbm],
        out_specs=vmem,
        scratch_shapes=[
            kept,
            pltpu.SemaphoreType.DMA((sides,)),
        ],
        compiler_params=pltpu.CompilerParams(vmem_limit_bytes=SPAN_MIB * 1024 * 1024),
        cost_estimate=pl.CostEstimate(flops=10**9, bytes_accessed=1, transcendentals=0),
        name="span",
    )(other, aux, acc, beta, key_rest, value_near)
    by_head = lax.all_to_all(span, "y", 0, 0, tiled=True)
    level_y = joined(by_head).astype(BF16)
    level_z = joined(to_all(level_y, "zq")).astype(BF16)

    upper = lax.axis_index("zh") == 1
    y = lax.axis_index("y")
    own_z = lax.axis_index("zh") * lax.axis_size("zq") + lax.axis_index("zq")
    partner_z = own_z ^ lax.axis_size("zq")
    rows = SPAN // (2 * lax.axis_size("zq"))
    query = lax.dynamic_index_in_dim(new_query[0], y, 0, keepdims=True).astype(F32)
    query = query * lax.rsqrt(jnp.sum(query * query, axis=-1, keepdims=True) + 1.0)
    pulled = dot(query, level_z) + 0.0

    def block_for(z):
        picked = lax.dynamic_slice_in_dim(level_z, z * rows, rows, 0)
        tail = jnp.zeros((SPAN // 2 - rows - 1, 2 * SPAN), BF16)
        return jnp.concatenate([picked, pulled.astype(BF16), tail], axis=0)

    send_rows = block_for(partner_z).reshape(SPAN, SPAN)
    sent = jnp.where(upper, send_rows, level_z[:, SPAN:])
    came = swapped(sent, "zh")
    late = jnp.where(upper, block_for(own_z), came.reshape(SPAN // 2, 2 * SPAN))
    early = jnp.where(upper, came, level_z[:, SPAN:])
    q_high, q_low = halves(query)
    kept = jnp.concatenate(
        [
            lax.dynamic_slice_in_dim(early, own_z * rows, rows, 0).astype(F32),
            dot(q_high, early) + dot(q_low, early),
        ],
        axis=0,
    )
    final = dot(late[: rows + 1, :SPAN], early) + late[: rows + 1, SPAN:].astype(F32) + kept
    each = rows // lax.axis_size("y")
    read = jnp.broadcast_to(final[None, rows:], (lax.axis_size("y"), 1, SPAN))
    packed = jnp.concatenate([final[:rows].reshape(-1, each, SPAN), read], axis=1)
    home = lax.all_to_all(packed, "y", 0, 0, tiled=True)
    raw = home[:, each]
    read_out = raw * lax.rsqrt(jnp.mean(raw * raw, axis=-1, keepdims=True) + 0.05) * read_gain
    return (home[:, :each].astype(BF16)[None], read_out[None])


def solution(mesh):
    y, x = 4, 4
    zq = 4
    zh = mesh.shape["sp"] // (zq * y)
    finer = Mesh(
        mesh.devices.reshape(mesh.shape["gr"], zh, zq, y, x, mesh.shape["tp"] // x),
        ("gr", "zh", "zq", "y", "x", "c"),
    )
    sp, tp = ("zh", "zq", "y"), ("x", "c")
    return jax.shard_map(
        shards,
        mesh=finer,
        in_specs=(
            P("gr", sp, tp),
            P(None, tp),
            P(None, tp),
            P(None, tp),
            P(tp),
            P(tp),
            P("gr", tp, None),
            P(),
        ),
        out_specs=(P("gr", tp, sp, None), P("gr", tp, None)),
        check_vma=False,
    )
```

```python
import functools

import jax
import jax.numpy as jnp
from jax import lax
from jax.experimental import pallas as pl
from jax.experimental.pallas import tpu as pltpu
from jax.sharding import Mesh
from jax.sharding import PartitionSpec as P

SPAN = 128
WIDE = 256
GROUP = 8
FIRST_MIB = 47
SPAN_MIB = 48
F32, BF16 = jnp.float32, jnp.bfloat16
NT = (((1,), (1,)), ((), ()))
NN = (((1,), (0,)), ((), ()))
TN = (((0,), (0,)), ((), ()))


def dot(a, b, dims=NN):
    return lax.dot_general(a.astype(BF16), b.astype(BF16), dims, preferred_element_type=F32)


def halves(a):
    high = a.astype(BF16)
    return high, (a - high.astype(F32)).astype(BF16)


def beta_sum(x_ref, aux_ref, side, heads):
    count, _, part = x_ref.shape
    total = None
    for j in range(count):
        start = pl.multiple_of((2 * j + side) * part, part)
        now = dot(x_ref[j], aux_ref[0:heads, pl.ds(start, part)], NT)
        total = now if total is None else total + now
    return total


def project(x_ref, weight_ref, out_ref, start):
    for n in range(0, weight_ref.shape[2], WIDE):
        total = None
        for j in range(x_ref.shape[0]):
            part = dot(x_ref[j], weight_ref[j, :, n : n + WIDE])
            total = part if total is None else total + part
        out_ref[:, start + n : start + n + WIDE] = total


def copied(src, dst, sem):
    made = pltpu.make_async_copy(src, dst, sem)
    made.start()
    return made


def first_kernel(
    x_ref, aux_ref, kw_ref, vw_ref, acc_ref, beta_ref, kw_out, kw_own, vw_own, sems,
):
    core = lax.axis_index("c")
    sides = range(x_ref.shape[0])
    cols = kw_ref.shape[2]
    keys = [copied(kw_ref.at[2 * j + core], kw_own.at[j], sems.at[0, j]) for j in sides]
    values = [copied(vw_ref.at[2 * j + core], vw_own.at[j], sems.at[1, j]) for j in sides]
    others = [copied(kw_ref.at[2 * j + 1 - core], kw_out.at[j], sems.at[2, j]) for j in sides]
    beta_ref[...] = beta_sum(x_ref, aux_ref, core, beta_ref.shape[1])
    for done in keys:
        done.wait()
    project(x_ref, kw_own, acc_ref, 0)
    for done in values:
        done.wait()
    project(x_ref, vw_own, acc_ref, cols)
    for done in others:
        done.wait()


def odd_rows(value, size):
    return jnp.concatenate(
        [value[r : r + size] for r in range(size, SPAN, 2 * size)], axis=0
    )


def woven(even, odd, size):
    parts = []
    for i in range(SPAN // (2 * size)):
        r = 2 * size * i
        parts.append(
            jnp.zeros((size, SPAN), F32) if even is None else even[r : r + size]
        )
        parts.append(odd[size * i : size * (i + 1)])
    return jnp.concatenate(parts, axis=0)


def span_kernel(
    full_len, x_ref, aux_ref, acc_ref, beta_ref, kw_ref, vw_ref, out_ref, vw_rest, sems,
):
    core = lax.axis_index("c")
    count, seg_len = x_ref.shape[:2]
    heads = out_ref.shape[0]
    cols = kw_ref.shape[2]
    rest = [
        copied(vw_ref.at[2 * j + 1 - core], vw_rest.at[j], sems.at[j]) for j in range(count)
    ]
    bias = aux_ref[heads : heads + 1, 0:heads]
    beta = beta_ref[...] + beta_sum(x_ref, aux_ref, 1 - core, heads)
    beta = jax.nn.sigmoid(beta + bias)
    keys = []
    for n in range(0, cols, WIDE):
        total = acc_ref[:, n : n + WIDE]
        for j in range(count):
            total = total + dot(x_ref[j], kw_ref[j, :, n : n + WIDE])
        keys.append(total.astype(BF16))

    row = lax.broadcasted_iota(jnp.int32, (SPAN, SPAN), 0)
    col = lax.broadcasted_iota(jnp.int32, (SPAN, SPAN), 1)
    apart = row ^ col
    lower = row > col
    eye = (row == col).astype(F32)
    place = lax.broadcasted_iota(jnp.int32, (1, SPAN), 1)
    later = (SPAN - 1 - place).astype(F32)

    jobs = [(h, s) for h in range(heads) for s in range(seg_len // SPAN)]
    per = WIDE // SPAN

    def cut(tiles, h, s):
        return tiles[h // per][s * SPAN : (s + 1) * SPAN, (h % per) * SPAN : (h % per + 1) * SPAN]

    gram = [dot(cut(keys, h, s), cut(keys, h, s), NT) for h, s in jobs]
    diag = [g * eye for g in gram]
    norm_row = [jnp.sum(d, axis=0, keepdims=True) for d in diag]
    scale_row = [lax.rsqrt(n + 1.0) for n in norm_row]
    beta_t = jnp.transpose(jnp.concatenate([beta, jnp.zeros((seg_len, SPAN - heads), F32)], axis=1))
    beta_row = [beta_t[h : h + 1, s * SPAN : (s + 1) * SPAN] for h, s in jobs]
    stack = jnp.concatenate(
        scale_row
        + [b * r for b, r in zip(beta_row, scale_row)]
        + [jnp.zeros((SPAN - 2 * len(jobs), SPAN), F32)],
        axis=0,
    )
    turned = jnp.transpose(stack)
    scale_col = [turned[:, i : i + 1] for i in range(len(jobs))]
    both_col = [turned[:, len(jobs) + i : len(jobs) + i + 1] for i in range(len(jobs))]
    low = [
        jnp.where(lower, g * b * r, 0.0) for g, b, r in zip(gram, both_col, scale_row)
    ]
    inv = [eye - jnp.where(apart == 1, lo, 0.0) for lo in low]
    log_step = [-aux_ref[heads + 1 : heads + 2, h : h + 1] / full_len for h, _ in jobs]
    key_row = [b * r for b, r in zip(beta_row, scale_row)]
    val_row = [b * jnp.exp(g * later) for b, g in zip(beta_row, log_step)]
    decay = [jnp.exp(g * SPAN + jnp.zeros((1, SPAN), F32)) for g in log_step]

    for done in rest:
        done.wait()
    pending = [(n, j) for n in range(0, cols, WIDE) for j in range(count)]
    value_acc = {n: acc_ref[:, cols + n : cols + n + WIDE] for n in range(0, cols, WIDE)}
    levels = SPAN.bit_length() - 2

    for level in range(1, levels + 1):
        size = 2**level
        inv_b = [t.astype(BF16) for t in inv]
        if size < 8:
            mask = (apart >> level) == 1
            low_m = [jnp.where(mask, lo, 0.0) for lo in low]
            mid = [dot(m, t) for m, t in zip(low_m, inv_b)]
            inv = [t - dot(tb, m) for t, tb, m in zip(inv, inv_b, mid)]
        else:
            mask = (odd_rows(apart, size) >> level) == 1
            low_m = [jnp.where(mask, odd_rows(lo, size), 0.0) for lo in low]
            mid = [woven(None, dot(m, t), size) for m, t in zip(low_m, inv_b)]
            inv = [
                woven(t, odd_rows(t, size) - dot(odd_rows(t, size), m), size)
                for t, m in zip(inv, mid)
            ]
        for _ in range(-(-len(pending) // (levels + 1 - level))):
            n, j = pending.pop(0)
            value_acc[n] = value_acc[n] + dot(x_ref[j], vw_rest[j, :, n : n + WIDE])
    values = [value_acc[n].astype(BF16) for n in range(0, cols, WIDE)]

    group = GROUP
    made = []
    for first in range(0, len(jobs), group):
        near = range(first, min(first + group, len(jobs)))
        split = [halves(inv[i]) for i in near]
        lows = [halves(low[i]) for i in near]
        left = [
            dot(jnp.concatenate([lo_h, lo_l], axis=1), jnp.concatenate([t_h, t_h], axis=0))
            + dot(lo_h, t_l)
            for (lo_h, lo_l), (t_h, t_l) in zip(lows, split)
        ]
        left = [((eye - inv[i]) - e).astype(BF16) for i, e in zip(near, left)]
        better = [inv[i] + dot(t_h, e) for i, (t_h, _), e in zip(near, split, left)]
        twice = [jnp.concatenate([cut(keys, *jobs[i])] * 2, axis=0) for i in near]
        x_key = [
            dot(jnp.concatenate(halves(t * key_row[i]), axis=1), k)
            for i, t, k in zip(near, better, twice)
        ]
        x_val = [
            dot(
                jnp.concatenate(halves(t * val_row[i]), axis=1),
                jnp.concatenate([cut(values, *jobs[i])] * 2, axis=0),
            )
            for i, t in zip(near, better)
        ]
        solved = [
            jnp.concatenate(
                halves(scale_col[i] * jnp.concatenate([xk * -decay[i], xv], axis=1)), axis=0
            )
            for i, xk, xv in zip(near, x_key, x_val)
        ]
        both = [dot(k, x, TN) for k, x in zip(twice, solved)]
        made += [
            (e[:, :SPAN] + eye * (decay[i] - 1.0), e[:, SPAN:]) for i, e in zip(near, both)
        ]

    for h in range(heads):
        total = None
        for s in range(seg_len // SPAN):
            change, write = made[h * (seg_len // SPAN) + s]
            now = jnp.concatenate([change, write], axis=1)
            total = now if total is None else now + total + dot(change, total)
        out_ref[h] = total.astype(BF16)


def last_kernel(home_ref, gain_ref, state_ref, read_ref):
    each = state_ref.shape[2]
    state_ref[0] = home_ref[:, :each].astype(BF16)
    raw = home_ref[:, each]
    mean = jnp.mean(raw * raw, axis=-1, keepdims=True)
    read_ref[0] = raw * lax.rsqrt(mean + 0.05) * gain_ref[...]


def joined(parts):
    total = parts[0].astype(F32)
    for j in range(1, parts.shape[0]):
        now = parts[j]
        total = total + now.astype(F32) + dot(now[:, :SPAN], total)
    return total


def to_all(value, axis):
    copies = jnp.broadcast_to(value[None], (lax.axis_size(axis), *value.shape))
    return lax.all_to_all(copies, axis, 0, 0, tiled=True)


def swapped(value, axis):
    return lax.ppermute(value, axis, [(0, 1), (1, 0)])


def shards(
    prompt, key_weight, value_weight, beta_weight, beta_bias, decay_rate, new_query, read_gain
):
    seg_len, part = prompt.shape[1], prompt.shape[2]
    heads = beta_weight.shape[1]
    tp = lax.axis_size(("x", "c"))
    sp = lax.axis_size(("zh", "zq", "y"))
    full_len = seg_len * sp
    mine = to_all(prompt[0], "x")
    other = swapped(mine, "c")
    vmem = pl.BlockSpec(memory_space=pltpu.VMEM)
    hbm = pl.BlockSpec(memory_space=pltpu.HBM)
    sides, cols = mine.shape[0], key_weight.shape[1]
    feat = tp * part
    aux = (
        jnp.pad(jnp.transpose(beta_weight).astype(F32), ((0, heads), (0, 0)))
        + jnp.pad(beta_bias[None], ((heads, heads - 1), (0, feat - heads)))
        + jnp.pad(decay_rate[None], ((heads + 1, heads - 2), (0, feat - heads)))
    )
    key_near = key_weight.reshape(tp, part, cols)
    value_near = value_weight.reshape(tp, part, cols)
    kept = pltpu.VMEM((sides, part, cols), BF16)
    acc, beta, key_rest = pl.pallas_call(
        first_kernel,
        out_shape=(
            jax.ShapeDtypeStruct((seg_len, 2 * cols), F32),
            jax.ShapeDtypeStruct((seg_len, heads), F32),
            jax.ShapeDtypeStruct((sides, part, cols), BF16),
        ),
        in_specs=[vmem, vmem, hbm, hbm],
        out_specs=[vmem] * 3,
        scratch_shapes=[kept, kept, pltpu.SemaphoreType.DMA((3, sides))],
        compiler_params=pltpu.CompilerParams(vmem_limit_bytes=FIRST_MIB * 1024 * 1024),
        cost_estimate=pl.CostEstimate(
            flops=4 * seg_len * sides * part * cols, bytes_accessed=1, transcendentals=0
        ),
        name="first",
    )(mine, aux, key_near, value_near)
    span = pl.pallas_call(
        functools.partial(span_kernel, full_len),
        out_shape=jax.ShapeDtypeStruct((heads, SPAN, 2 * SPAN), BF16),
        in_specs=[vmem] * 5 + [hbm],
        out_specs=vmem,
        scratch_shapes=[
            kept,
            pltpu.SemaphoreType.DMA((sides,)),
        ],
        compiler_params=pltpu.CompilerParams(vmem_limit_bytes=SPAN_MIB * 1024 * 1024),
        cost_estimate=pl.CostEstimate(flops=10**9, bytes_accessed=1, transcendentals=0),
        name="span",
    )(other, aux, acc, beta, key_rest, value_near)
    by_head = lax.all_to_all(span, "y", 0, 0, tiled=True)
    level_y = joined(by_head).astype(BF16)
    level_z = joined(to_all(level_y, "zq")).astype(BF16)

    upper = lax.axis_index("zh") == 1
    y = lax.axis_index("y")
    own_z = lax.axis_index("zh") * lax.axis_size("zq") + lax.axis_index("zq")
    partner_z = own_z ^ lax.axis_size("zq")
    rows = SPAN // (2 * lax.axis_size("zq"))
    query = lax.dynamic_index_in_dim(new_query[0], y, 0, keepdims=True).astype(F32)
    query = query * lax.rsqrt(jnp.sum(query * query, axis=-1, keepdims=True) + 1.0)
    pulled = dot(query, level_z) + 0.0

    def block_for(z):
        picked = lax.dynamic_slice_in_dim(level_z, z * rows, rows, 0)
        tail = jnp.zeros((SPAN // 2 - rows - 1, 2 * SPAN), BF16)
        return jnp.concatenate([picked, pulled.astype(BF16), tail], axis=0)

    send_rows = block_for(partner_z).reshape(SPAN, SPAN)
    sent = jnp.where(upper, send_rows, level_z[:, SPAN:])
    came = swapped(sent, "zh")
    late = jnp.where(upper, block_for(own_z), came.reshape(SPAN // 2, 2 * SPAN))
    early = jnp.where(upper, came, level_z[:, SPAN:])
    q_high, q_low = halves(query)
    kept = jnp.concatenate(
        [
            lax.dynamic_slice_in_dim(early, own_z * rows, rows, 0).astype(F32),
            dot(q_high, early) + dot(q_low, early),
        ],
        axis=0,
    )
    final = dot(late[: rows + 1, :SPAN], early) + late[: rows + 1, SPAN:].astype(F32) + kept
    each = rows // lax.axis_size("y")
    read = jnp.broadcast_to(final[None, rows:], (lax.axis_size("y"), 1, SPAN))
    packed = jnp.concatenate([final[:rows].reshape(-1, each, SPAN), read], axis=1)
    home = lax.all_to_all(packed, "y", 0, 0, tiled=True)
    return pl.pallas_call(
        last_kernel,
        out_shape=(
            jax.ShapeDtypeStruct((1, heads, each, SPAN), BF16),
            jax.ShapeDtypeStruct((1, heads, SPAN), F32),
        ),
        in_specs=[vmem] * 2,
        out_specs=[vmem] * 2,
        compiler_params=pltpu.CompilerParams(vmem_limit_bytes=4 * 1024 * 1024),
        name="last",
    )(home, read_gain[None])


def solution(mesh):
    y, x = 4, 4
    zq = 4
    zh = mesh.shape["sp"] // (zq * y)
    finer = Mesh(
        mesh.devices.reshape(mesh.shape["gr"], zh, zq, y, x, mesh.shape["tp"] // x),
        ("gr", "zh", "zq", "y", "x", "c"),
    )
    sp, tp = ("zh", "zq", "y"), ("x", "c")
    return jax.shard_map(
        shards,
        mesh=finer,
        in_specs=(
            P("gr", sp, tp),
            P(None, tp),
            P(None, tp),
            P(None, tp),
            P(tp),
            P(tp),
            P("gr", tp, None),
            P(),
        ),
        out_specs=(P("gr", tp, sp, None), P("gr", tp, None)),
        check_vma=False,
    )
```

```python
import functools

import jax
import jax.numpy as jnp
from jax import lax
from jax.experimental import pallas as pl
from jax.experimental.pallas import tpu as pltpu
from jax.sharding import Mesh
from jax.sharding import PartitionSpec as P

SPAN = 128
WIDE = 256
GROUP = 8
FIRST_MIB = 47
SPAN_MIB = 48
F32, BF16 = jnp.float32, jnp.bfloat16
NT = (((1,), (1,)), ((), ()))
NN = (((1,), (0,)), ((), ()))
TN = (((0,), (0,)), ((), ()))


def dot(a, b, dims=NN):
    return lax.dot_general(a.astype(BF16), b.astype(BF16), dims, preferred_element_type=F32)


def halves(a):
    high = a.astype(BF16)
    return high, (a - high.astype(F32)).astype(BF16)


def beta_sum(x_ref, aux_ref, side, heads):
    count, _, part = x_ref.shape
    total = None
    for j in range(count):
        start = pl.multiple_of((2 * j + side) * part, part)
        now = dot(x_ref[j], aux_ref[0:heads, pl.ds(start, part)], NT)
        total = now if total is None else total + now
    return total


def project(x_ref, weight_ref, out_ref, start):
    for n in range(0, weight_ref.shape[2], WIDE):
        total = None
        for j in range(x_ref.shape[0]):
            part = dot(x_ref[j], weight_ref[j, :, n : n + WIDE])
            total = part if total is None else total + part
        out_ref[:, start + n : start + n + WIDE] = total


def copied(src, dst, sem):
    made = pltpu.make_async_copy(src, dst, sem)
    made.start()
    return made


def first_kernel(
    x_ref, aux_ref, kw_ref, vw_ref, acc_ref, beta_ref, kw_out, kw_own, vw_own, sems,
):
    core = lax.axis_index("c")
    sides = range(x_ref.shape[0])
    cols = kw_ref.shape[2]
    keys = [copied(kw_ref.at[2 * j + core], kw_own.at[j], sems.at[0, j]) for j in sides]
    values = [copied(vw_ref.at[2 * j + core], vw_own.at[j], sems.at[1, j]) for j in sides]
    others = [copied(kw_ref.at[2 * j + 1 - core], kw_out.at[j], sems.at[2, j]) for j in sides]
    beta_ref[...] = beta_sum(x_ref, aux_ref, core, beta_ref.shape[1])
    for done in keys:
        done.wait()
    project(x_ref, kw_own, acc_ref, 0)
    for done in values:
        done.wait()
    project(x_ref, vw_own, acc_ref, cols)
    for done in others:
        done.wait()


def odd_rows(value, size):
    return jnp.concatenate(
        [value[r : r + size] for r in range(size, SPAN, 2 * size)], axis=0
    )


def woven(even, odd, size):
    parts = []
    for i in range(SPAN // (2 * size)):
        r = 2 * size * i
        parts.append(
            jnp.zeros((size, SPAN), F32) if even is None else even[r : r + size]
        )
        parts.append(odd[size * i : size * (i + 1)])
    return jnp.concatenate(parts, axis=0)


def span_kernel(
    full_len, x_ref, aux_ref, acc_ref, beta_ref, kw_ref, vw_ref, out_ref, query_ref, vw_rest, sems,
):
    core = lax.axis_index("c")
    count, seg_len = x_ref.shape[:2]
    heads = out_ref.shape[0]
    cols = kw_ref.shape[2]
    rest = [
        copied(vw_ref.at[2 * j + 1 - core], vw_rest.at[j], sems.at[j]) for j in range(count)
    ]
    query = aux_ref[0:heads, 2 * count * x_ref.shape[2] :]
    query_ref[...] = query * lax.rsqrt(jnp.sum(query * query, axis=-1, keepdims=True) + 1.0)
    bias = aux_ref[heads : heads + 1, 0:heads]
    beta = beta_ref[...] + beta_sum(x_ref, aux_ref, 1 - core, heads)
    beta = jax.nn.sigmoid(beta + bias)
    keys = []
    for n in range(0, cols, WIDE):
        total = acc_ref[:, n : n + WIDE]
        for j in range(count):
            total = total + dot(x_ref[j], kw_ref[j, :, n : n + WIDE])
        keys.append(total.astype(BF16))

    row = lax.broadcasted_iota(jnp.int32, (SPAN, SPAN), 0)
    col = lax.broadcasted_iota(jnp.int32, (SPAN, SPAN), 1)
    apart = row ^ col
    lower = row > col
    eye = (row == col).astype(F32)
    place = lax.broadcasted_iota(jnp.int32, (1, SPAN), 1)
    later = (SPAN - 1 - place).astype(F32)

    jobs = [(h, s) for h in range(heads) for s in range(seg_len // SPAN)]
    per = WIDE // SPAN

    def cut(tiles, h, s):
        return tiles[h // per][s * SPAN : (s + 1) * SPAN, (h % per) * SPAN : (h % per + 1) * SPAN]

    gram = [dot(cut(keys, h, s), cut(keys, h, s), NT) for h, s in jobs]
    diag = [g * eye for g in gram]
    norm_row = [jnp.sum(d, axis=0, keepdims=True) for d in diag]
    scale_row = [lax.rsqrt(n + 1.0) for n in norm_row]
    beta_t = jnp.transpose(jnp.concatenate([beta, jnp.zeros((seg_len, SPAN - heads), F32)], axis=1))
    beta_row = [beta_t[h : h + 1, s * SPAN : (s + 1) * SPAN] for h, s in jobs]
    stack = jnp.concatenate(
        scale_row
        + [b * r for b, r in zip(beta_row, scale_row)]
        + [jnp.zeros((SPAN - 2 * len(jobs), SPAN), F32)],
        axis=0,
    )
    turned = jnp.transpose(stack)
    scale_col = [turned[:, i : i + 1] for i in range(len(jobs))]
    both_col = [turned[:, len(jobs) + i : len(jobs) + i + 1] for i in range(len(jobs))]
    low = [
        jnp.where(lower, g * b * r, 0.0) for g, b, r in zip(gram, both_col, scale_row)
    ]
    inv = [eye - jnp.where(apart == 1, lo, 0.0) for lo in low]
    log_step = [-aux_ref[heads + 1 : heads + 2, h : h + 1] / full_len for h, _ in jobs]
    key_row = [b * r for b, r in zip(beta_row, scale_row)]
    val_row = [b * jnp.exp(g * later) for b, g in zip(beta_row, log_step)]
    decay = [jnp.exp(g * SPAN + jnp.zeros((1, SPAN), F32)) for g in log_step]

    for done in rest:
        done.wait()
    pending = [(n, j) for n in range(0, cols, WIDE) for j in range(count)]
    value_acc = {n: acc_ref[:, cols + n : cols + n + WIDE] for n in range(0, cols, WIDE)}
    levels = SPAN.bit_length() - 2

    for level in range(1, levels + 1):
        size = 2**level
        inv_b = [t.astype(BF16) for t in inv]
        if size < 8:
            mask = (apart >> level) == 1
            low_m = [jnp.where(mask, lo, 0.0) for lo in low]
            mid = [dot(m, t) for m, t in zip(low_m, inv_b)]
            inv = [t - dot(tb, m) for t, tb, m in zip(inv, inv_b, mid)]
        else:
            mask = (odd_rows(apart, size) >> level) == 1
            low_m = [jnp.where(mask, odd_rows(lo, size), 0.0) for lo in low]
            mid = [woven(None, dot(m, t), size) for m, t in zip(low_m, inv_b)]
            inv = [
                woven(t, odd_rows(t, size) - dot(odd_rows(t, size), m), size)
                for t, m in zip(inv, mid)
            ]
        for _ in range(-(-len(pending) // (levels + 1 - level))):
            n, j = pending.pop(0)
            value_acc[n] = value_acc[n] + dot(x_ref[j], vw_rest[j, :, n : n + WIDE])
    values = [value_acc[n].astype(BF16) for n in range(0, cols, WIDE)]

    group = GROUP
    made = []
    for first in range(0, len(jobs), group):
        near = range(first, min(first + group, len(jobs)))
        split = [halves(inv[i]) for i in near]
        lows = [halves(low[i]) for i in near]
        left = [
            dot(jnp.concatenate([lo_h, lo_l], axis=1), jnp.concatenate([t_h, t_h], axis=0))
            + dot(lo_h, t_l)
            for (lo_h, lo_l), (t_h, t_l) in zip(lows, split)
        ]
        left = [((eye - inv[i]) - e).astype(BF16) for i, e in zip(near, left)]
        better = [inv[i] + dot(t_h, e) for i, (t_h, _), e in zip(near, split, left)]
        twice = [jnp.concatenate([cut(keys, *jobs[i])] * 2, axis=0) for i in near]
        x_key = [
            dot(jnp.concatenate(halves(t * key_row[i]), axis=1), k)
            for i, t, k in zip(near, better, twice)
        ]
        x_val = [
            dot(
                jnp.concatenate(halves(t * val_row[i]), axis=1),
                jnp.concatenate([cut(values, *jobs[i])] * 2, axis=0),
            )
            for i, t in zip(near, better)
        ]
        solved = [
            jnp.concatenate(
                halves(scale_col[i] * jnp.concatenate([xk * -decay[i], xv], axis=1)), axis=0
            )
            for i, xk, xv in zip(near, x_key, x_val)
        ]
        both = [dot(k, x, TN) for k, x in zip(twice, solved)]
        made += [
            (e[:, :SPAN] + eye * (decay[i] - 1.0), e[:, SPAN:]) for i, e in zip(near, both)
        ]

    for h in range(heads):
        total = None
        for s in range(seg_len // SPAN):
            change, write = made[h * (seg_len // SPAN) + s]
            now = jnp.concatenate([change, write], axis=1)
            total = now if total is None else now + total + dot(change, total)
        out_ref[h] = total.astype(BF16)


def rows_at(z, rows):
    return pl.ds(pl.multiple_of(z * rows, rows), rows)


def merge_kernel(quads, rows, parts_ref, query_ref, sent_ref, own_ref, level_ref):
    upper = lax.axis_index("zh") == 1
    own_z = lax.axis_index("zh") * quads + lax.axis_index("zq")
    partner_z = own_z ^ quads
    total = parts_ref[0].astype(F32)
    for j in range(1, parts_ref.shape[0]):
        now = parts_ref[j]
        total = total + now.astype(F32) + dot(now[:, :SPAN], total)
    level = total.astype(BF16)
    level_ref[...] = level
    query = jnp.broadcast_to(query_ref[pl.ds(lax.axis_index("y"), 1), :], (rows, SPAN))
    pulled = dot(query, level).astype(BF16)
    pulled = jnp.concatenate([pulled[:, :SPAN], pulled[:, SPAN:]], axis=0)

    def write(ref, z):
        picked = level_ref[rows_at(z, rows), :]
        ref[0:rows] = picked[:, :SPAN]
        ref[rows : 2 * rows] = picked[:, SPAN:]
        ref[2 * rows : 4 * rows] = pulled

    write(own_ref, own_z)

    @pl.when(upper)
    def _():
        write(sent_ref, partner_z)
        sent_ref[4 * rows :] = jnp.zeros((SPAN - 4 * rows, SPAN), BF16)

    @pl.when(jnp.logical_not(upper))
    def _():
        sent_ref[...] = level[:, SPAN:]


def finish_kernel(quads, rows, came_ref, own_ref, level_ref, query_ref, packed_ref, early_s):
    upper = lax.axis_index("zh") == 1
    own_z = lax.axis_index("zh") * quads + lax.axis_index("zq")
    came = came_ref[...].astype(F32)
    early = jnp.where(upper, came, level_ref[:, SPAN:].astype(F32))
    late = jnp.where(upper, own_ref[...].astype(F32), came[: 4 * rows])
    early_s[...] = early
    change = jnp.concatenate([late[:rows], late[2 * rows : 3 * rows]], axis=0)
    write = jnp.concatenate([late[rows : 2 * rows], late[3 * rows :]], axis=0)
    query = jnp.broadcast_to(query_ref[pl.ds(lax.axis_index("y"), 1), :], (rows, SPAN))
    high, low = halves(query)
    kept = jnp.concatenate(
        [early_s[rows_at(own_z, rows), :], dot(high, early) + dot(low, early)], axis=0
    )
    final = dot(change, early) + write + kept
    ways, each = packed_ref.shape[0], packed_ref.shape[1] - 1
    for j in range(ways):
        packed_ref[j, 0:each] = final[each * j : each * (j + 1)]
        packed_ref[j, each : each + 1] = final[rows : rows + 1]


def last_kernel(home_ref, gain_ref, state_ref, read_ref):
    each = state_ref.shape[2]
    state_ref[0] = home_ref[:, :each].astype(BF16)
    raw = home_ref[:, each]
    mean = jnp.mean(raw * raw, axis=-1, keepdims=True)
    read_ref[0] = raw * lax.rsqrt(mean + 0.05) * gain_ref[...]


def joined(parts):
    total = parts[0].astype(F32)
    for j in range(1, parts.shape[0]):
        now = parts[j]
        total = total + now.astype(F32) + dot(now[:, :SPAN], total)
    return total


def to_all(value, axis):
    copies = jnp.broadcast_to(value[None], (lax.axis_size(axis), *value.shape))
    return lax.all_to_all(copies, axis, 0, 0, tiled=True)


def swapped(value, axis):
    return lax.ppermute(value, axis, [(0, 1), (1, 0)])


def shards(
    prompt, key_weight, value_weight, beta_weight, beta_bias, decay_rate, new_query, read_gain
):
    seg_len, part = prompt.shape[1], prompt.shape[2]
    heads = beta_weight.shape[1]
    tp = lax.axis_size(("x", "c"))
    sp = lax.axis_size(("zh", "zq", "y"))
    full_len = seg_len * sp
    mine = to_all(prompt[0], "x")
    other = swapped(mine, "c")
    vmem = pl.BlockSpec(memory_space=pltpu.VMEM)
    hbm = pl.BlockSpec(memory_space=pltpu.HBM)
    sides, cols = mine.shape[0], key_weight.shape[1]
    feat = tp * part
    aux = (
        jnp.pad(jnp.transpose(beta_weight).astype(F32), ((0, heads), (0, SPAN)))
        + jnp.pad(beta_bias[None], ((heads, heads - 1), (0, feat + SPAN - heads)))
        + jnp.pad(decay_rate[None], ((heads + 1, heads - 2), (0, feat + SPAN - heads)))
        + jnp.pad(new_query[0].astype(F32), ((0, heads), (feat, 0)))
    )
    key_near = key_weight.reshape(tp, part, cols)
    value_near = value_weight.reshape(tp, part, cols)
    kept = pltpu.VMEM((sides, part, cols), BF16)
    acc, beta, key_rest = pl.pallas_call(
        first_kernel,
        out_shape=(
            jax.ShapeDtypeStruct((seg_len, 2 * cols), F32),
            jax.ShapeDtypeStruct((seg_len, heads), F32),
            jax.ShapeDtypeStruct((sides, part, cols), BF16),
        ),
        in_specs=[vmem, vmem, hbm, hbm],
        out_specs=[vmem] * 3,
        scratch_shapes=[kept, kept, pltpu.SemaphoreType.DMA((3, sides))],
        compiler_params=pltpu.CompilerParams(vmem_limit_bytes=FIRST_MIB * 1024 * 1024),
        cost_estimate=pl.CostEstimate(
            flops=4 * seg_len * sides * part * cols, bytes_accessed=1, transcendentals=0
        ),
        name="first",
    )(mine, aux, key_near, value_near)
    span, query = pl.pallas_call(
        functools.partial(span_kernel, full_len),
        out_shape=(
            jax.ShapeDtypeStruct((heads, SPAN, 2 * SPAN), BF16),
            jax.ShapeDtypeStruct((heads, SPAN), F32),
        ),
        in_specs=[vmem] * 5 + [hbm],
        out_specs=[vmem] * 2,
        scratch_shapes=[
            kept,
            pltpu.SemaphoreType.DMA((sides,)),
        ],
        compiler_params=pltpu.CompilerParams(vmem_limit_bytes=SPAN_MIB * 1024 * 1024),
        cost_estimate=pl.CostEstimate(flops=10**9, bytes_accessed=1, transcendentals=0),
        name="span",
    )(other, aux, acc, beta, key_rest, value_near)
    by_head = lax.all_to_all(span, "y", 0, 0, tiled=True)
    level_y = joined(by_head).astype(BF16)
    parts = to_all(level_y, "zq")
    quads, ways = lax.axis_size("zq"), lax.axis_size("y")
    rows = SPAN // (2 * quads)
    each = rows // ways
    little = pltpu.CompilerParams(vmem_limit_bytes=4 * 1024 * 1024)
    block = jax.ShapeDtypeStruct((SPAN, SPAN), BF16)
    sent, own, level_z = pl.pallas_call(
        functools.partial(merge_kernel, quads, rows),
        out_shape=(
            block,
            jax.ShapeDtypeStruct((4 * rows, SPAN), BF16),
            jax.ShapeDtypeStruct((SPAN, 2 * SPAN), BF16),
        ),
        in_specs=[vmem] * 2,
        out_specs=[vmem] * 3,
        compiler_params=little,
        name="merge",
    )(parts, query)
    packed = pl.pallas_call(
        functools.partial(finish_kernel, quads, rows),
        out_shape=jax.ShapeDtypeStruct((ways, each + 1, SPAN), F32),
        in_specs=[vmem] * 4,
        out_specs=vmem,
        scratch_shapes=[pltpu.VMEM((SPAN, SPAN), F32)],
        compiler_params=little,
        name="finish",
    )(swapped(sent, "zh"), own, level_z, query)
    home = lax.all_to_all(packed, "y", 0, 0, tiled=True)
    return pl.pallas_call(
        last_kernel,
        out_shape=(
            jax.ShapeDtypeStruct((1, heads, each, SPAN), BF16),
            jax.ShapeDtypeStruct((1, heads, SPAN), F32),
        ),
        in_specs=[vmem] * 2,
        out_specs=[vmem] * 2,
        compiler_params=pltpu.CompilerParams(vmem_limit_bytes=4 * 1024 * 1024),
        name="last",
    )(home, read_gain[None])


def solution(mesh):
    y, x = 4, 4
    zq = 4
    zh = mesh.shape["sp"] // (zq * y)
    finer = Mesh(
        mesh.devices.reshape(mesh.shape["gr"], zh, zq, y, x, mesh.shape["tp"] // x),
        ("gr", "zh", "zq", "y", "x", "c"),
    )
    sp, tp = ("zh", "zq", "y"), ("x", "c")
    return jax.shard_map(
        shards,
        mesh=finer,
        in_specs=(
            P("gr", sp, tp),
            P(None, tp),
            P(None, tp),
            P(None, tp),
            P(tp),
            P(tp),
            P("gr", tp, None),
            P(),
        ),
        out_specs=(P("gr", tp, sp, None), P("gr", tp, None)),
        check_vma=False,
    )
```

```python
import functools

import jax
import jax.numpy as jnp
from jax import lax
from jax.experimental import pallas as pl
from jax.experimental.pallas import tpu as pltpu
from jax.sharding import Mesh
from jax.sharding import PartitionSpec as P

SPAN = 128
WIDE = 256
GROUP = 8
FIRST_MIB = 47
SPAN_MIB = 48
F32, BF16 = jnp.float32, jnp.bfloat16
NT = (((1,), (1,)), ((), ()))
NN = (((1,), (0,)), ((), ()))
TN = (((0,), (0,)), ((), ()))


def dot(a, b, dims=NN):
    return lax.dot_general(a.astype(BF16), b.astype(BF16), dims, preferred_element_type=F32)


def halves(a):
    high = a.astype(BF16)
    return high, (a - high.astype(F32)).astype(BF16)


def beta_sum(x_ref, aux_ref, side, heads):
    count, _, part = x_ref.shape
    total = None
    for j in range(count):
        start = pl.multiple_of((2 * j + side) * part, part)
        now = dot(x_ref[j], aux_ref[0:heads, pl.ds(start, part)], NT)
        total = now if total is None else total + now
    return total


def project(x_ref, weight_ref, out_ref, start):
    for n in range(0, weight_ref.shape[2], WIDE):
        total = None
        for j in range(x_ref.shape[0]):
            part = dot(x_ref[j], weight_ref[j, :, n : n + WIDE])
            total = part if total is None else total + part
        out_ref[:, start + n : start + n + WIDE] = total


def copied(src, dst, sem):
    made = pltpu.make_async_copy(src, dst, sem)
    made.start()
    return made


def first_kernel(
    x_ref, aux_ref, kw_ref, vw_ref, acc_ref, beta_ref, kw_out, query_ref, kw_own, vw_own, sems,
):
    core = lax.axis_index("c")
    sides = range(x_ref.shape[0])
    cols = kw_ref.shape[2]
    keys = [copied(kw_ref.at[2 * j + core], kw_own.at[j], sems.at[0, j]) for j in sides]
    values = [copied(vw_ref.at[2 * j + core], vw_own.at[j], sems.at[1, j]) for j in sides]
    others = [copied(kw_ref.at[2 * j + 1 - core], kw_out.at[j], sems.at[2, j]) for j in sides]
    beta_ref[...] = beta_sum(x_ref, aux_ref, core, beta_ref.shape[1])
    query = aux_ref[0 : query_ref.shape[0], kw_ref.shape[0] * kw_ref.shape[1] :]
    query_ref[...] = query * lax.rsqrt(jnp.sum(query * query, axis=-1, keepdims=True) + 1.0)
    for done in keys:
        done.wait()
    project(x_ref, kw_own, acc_ref, 0)
    for done in values:
        done.wait()
    project(x_ref, vw_own, acc_ref, cols)
    for done in others:
        done.wait()


def odd_rows(value, size):
    return jnp.concatenate(
        [value[r : r + size] for r in range(size, SPAN, 2 * size)], axis=0
    )


def woven(even, odd, size):
    parts = []
    for i in range(SPAN // (2 * size)):
        r = 2 * size * i
        parts.append(
            jnp.zeros((size, SPAN), F32) if even is None else even[r : r + size]
        )
        parts.append(odd[size * i : size * (i + 1)])
    return jnp.concatenate(parts, axis=0)


def span_kernel(
    full_len, x_ref, aux_ref, acc_ref, beta_ref, kw_ref, vw_ref, out_ref, vw_rest, sems,
):
    core = lax.axis_index("c")
    count, seg_len = x_ref.shape[:2]
    heads = out_ref.shape[0]
    cols = kw_ref.shape[2]
    rest = [
        copied(vw_ref.at[2 * j + 1 - core], vw_rest.at[j], sems.at[j]) for j in range(count)
    ]
    bias = aux_ref[heads : heads + 1, 0:heads]
    beta = beta_ref[...] + beta_sum(x_ref, aux_ref, 1 - core, heads)
    beta = jax.nn.sigmoid(beta + bias)
    keys = []
    for n in range(0, cols, WIDE):
        total = acc_ref[:, n : n + WIDE]
        for j in range(count):
            total = total + dot(x_ref[j], kw_ref[j, :, n : n + WIDE])
        keys.append(total.astype(BF16))

    row = lax.broadcasted_iota(jnp.int32, (SPAN, SPAN), 0)
    col = lax.broadcasted_iota(jnp.int32, (SPAN, SPAN), 1)
    apart = row ^ col
    lower = row > col
    eye = (row == col).astype(F32)
    place = lax.broadcasted_iota(jnp.int32, (1, SPAN), 1)
    later = (SPAN - 1 - place).astype(F32)

    jobs = [(h, s) for h in range(heads) for s in range(seg_len // SPAN)]
    per = WIDE // SPAN

    def cut(tiles, h, s):
        return tiles[h // per][s * SPAN : (s + 1) * SPAN, (h % per) * SPAN : (h % per + 1) * SPAN]

    gram = [dot(cut(keys, h, s), cut(keys, h, s), NT) for h, s in jobs]
    diag = [g * eye for g in gram]
    norm_row = [jnp.sum(d, axis=0, keepdims=True) for d in diag]
    scale_row = [lax.rsqrt(n + 1.0) for n in norm_row]
    beta_t = jnp.transpose(jnp.concatenate([beta, jnp.zeros((seg_len, SPAN - heads), F32)], axis=1))
    beta_row = [beta_t[h : h + 1, s * SPAN : (s + 1) * SPAN] for h, s in jobs]
    stack = jnp.concatenate(
        scale_row
        + [b * r for b, r in zip(beta_row, scale_row)]
        + [jnp.zeros((SPAN - 2 * len(jobs), SPAN), F32)],
        axis=0,
    )
    turned = jnp.transpose(stack)
    scale_col = [turned[:, i : i + 1] for i in range(len(jobs))]
    both_col = [turned[:, len(jobs) + i : len(jobs) + i + 1] for i in range(len(jobs))]
    low = [
        jnp.where(lower, g * b * r, 0.0) for g, b, r in zip(gram, both_col, scale_row)
    ]
    inv = [eye - jnp.where(apart == 1, lo, 0.0) for lo in low]
    log_step = [-aux_ref[heads + 1 : heads + 2, h : h + 1] / full_len for h, _ in jobs]
    key_row = [b * r for b, r in zip(beta_row, scale_row)]
    val_row = [b * jnp.exp(g * later) for b, g in zip(beta_row, log_step)]
    decay = [jnp.exp(g * SPAN + jnp.zeros((1, SPAN), F32)) for g in log_step]

    for done in rest:
        done.wait()
    pending = [(n, j) for n in range(0, cols, WIDE) for j in range(count)]
    value_acc = {n: acc_ref[:, cols + n : cols + n + WIDE] for n in range(0, cols, WIDE)}
    levels = SPAN.bit_length() - 2

    for level in range(1, levels + 1):
        size = 2**level
        inv_b = [t.astype(BF16) for t in inv]
        if size < 8:
            mask = (apart >> level) == 1
            low_m = [jnp.where(mask, lo, 0.0) for lo in low]
            mid = [dot(m, t) for m, t in zip(low_m, inv_b)]
            inv = [t - dot(tb, m) for t, tb, m in zip(inv, inv_b, mid)]
        else:
            mask = (odd_rows(apart, size) >> level) == 1
            low_m = [jnp.where(mask, odd_rows(lo, size), 0.0) for lo in low]
            mid = [woven(None, dot(m, t), size) for m, t in zip(low_m, inv_b)]
            inv = [
                woven(t, odd_rows(t, size) - dot(odd_rows(t, size), m), size)
                for t, m in zip(inv, mid)
            ]
        for _ in range(-(-len(pending) // (levels + 1 - level))):
            n, j = pending.pop(0)
            value_acc[n] = value_acc[n] + dot(x_ref[j], vw_rest[j, :, n : n + WIDE])
    values = [value_acc[n].astype(BF16) for n in range(0, cols, WIDE)]

    group = GROUP
    made = []
    for first in range(0, len(jobs), group):
        near = range(first, min(first + group, len(jobs)))
        split = [halves(inv[i]) for i in near]
        lows = [halves(low[i]) for i in near]
        left = [
            dot(jnp.concatenate([lo_h, lo_l], axis=1), jnp.concatenate([t_h, t_h], axis=0))
            + dot(lo_h, t_l)
            for (lo_h, lo_l), (t_h, t_l) in zip(lows, split)
        ]
        left = [((eye - inv[i]) - e).astype(BF16) for i, e in zip(near, left)]
        better = [inv[i] + dot(t_h, e) for i, (t_h, _), e in zip(near, split, left)]
        twice = [jnp.concatenate([cut(keys, *jobs[i])] * 2, axis=0) for i in near]
        x_key = [
            dot(jnp.concatenate(halves(t * key_row[i]), axis=1), k)
            for i, t, k in zip(near, better, twice)
        ]
        x_val = [
            dot(
                jnp.concatenate(halves(t * val_row[i]), axis=1),
                jnp.concatenate([cut(values, *jobs[i])] * 2, axis=0),
            )
            for i, t in zip(near, better)
        ]
        solved = [
            jnp.concatenate(
                halves(scale_col[i] * jnp.concatenate([xk * -decay[i], xv], axis=1)), axis=0
            )
            for i, xk, xv in zip(near, x_key, x_val)
        ]
        both = [dot(k, x, TN) for k, x in zip(twice, solved)]
        made += [
            (e[:, :SPAN] + eye * (decay[i] - 1.0), e[:, SPAN:]) for i, e in zip(near, both)
        ]

    for h in range(heads):
        total = None
        for s in range(seg_len // SPAN):
            change, write = made[h * (seg_len // SPAN) + s]
            now = jnp.concatenate([change, write], axis=1)
            total = now if total is None else now + total + dot(change, total)
        out_ref[h] = total.astype(BF16)


def rows_at(z, rows):
    return pl.ds(pl.multiple_of(z * rows, rows), rows)


def merge_kernel(quads, rows, parts_ref, query_ref, sent_ref, own_ref, level_ref):
    upper = lax.axis_index("zh") == 1
    own_z = lax.axis_index("zh") * quads + lax.axis_index("zq")
    partner_z = own_z ^ quads
    total = parts_ref[0].astype(F32)
    for j in range(1, parts_ref.shape[0]):
        now = parts_ref[j]
        total = total + now.astype(F32) + dot(now[:, :SPAN], total)
    level = total.astype(BF16)
    level_ref[...] = level
    query = jnp.broadcast_to(query_ref[pl.ds(lax.axis_index("y"), 1), :], (rows, SPAN))
    pulled = dot(query, level).astype(BF16)
    pulled = jnp.concatenate([pulled[:, :SPAN], pulled[:, SPAN:]], axis=0)

    def write(ref, z):
        picked = level_ref[rows_at(z, rows), :]
        ref[0:rows] = picked[:, :SPAN]
        ref[rows : 2 * rows] = picked[:, SPAN:]
        ref[2 * rows : 4 * rows] = pulled

    write(own_ref, own_z)

    @pl.when(upper)
    def _():
        write(sent_ref, partner_z)
        sent_ref[4 * rows :] = jnp.zeros((SPAN - 4 * rows, SPAN), BF16)

    @pl.when(jnp.logical_not(upper))
    def _():
        sent_ref[...] = level[:, SPAN:]


def finish_kernel(quads, rows, came_ref, own_ref, level_ref, query_ref, packed_ref, early_s):
    upper = lax.axis_index("zh") == 1
    own_z = lax.axis_index("zh") * quads + lax.axis_index("zq")
    came = came_ref[...].astype(F32)
    early = jnp.where(upper, came, level_ref[:, SPAN:].astype(F32))
    late = jnp.where(upper, own_ref[...].astype(F32), came[: 4 * rows])
    early_s[...] = early
    change = jnp.concatenate([late[:rows], late[2 * rows : 3 * rows]], axis=0)
    write = jnp.concatenate([late[rows : 2 * rows], late[3 * rows :]], axis=0)
    query = jnp.broadcast_to(query_ref[pl.ds(lax.axis_index("y"), 1), :], (rows, SPAN))
    high, low = halves(query)
    kept = jnp.concatenate(
        [early_s[rows_at(own_z, rows), :], dot(high, early) + dot(low, early)], axis=0
    )
    final = dot(change, early) + write + kept
    ways, each = packed_ref.shape[0], packed_ref.shape[1] - 1
    for j in range(ways):
        packed_ref[j, 0:each] = final[each * j : each * (j + 1)]
        packed_ref[j, each : each + 1] = final[rows : rows + 1]


def last_kernel(home_ref, gain_ref, state_ref, read_ref):
    each = state_ref.shape[2]
    state_ref[0] = home_ref[:, :each].astype(BF16)
    raw = home_ref[:, each]
    mean = jnp.mean(raw * raw, axis=-1, keepdims=True)
    read_ref[0] = raw * lax.rsqrt(mean + 0.05) * gain_ref[...]


def joined(parts):
    total = parts[0].astype(F32)
    for j in range(1, parts.shape[0]):
        now = parts[j]
        total = total + now.astype(F32) + dot(now[:, :SPAN], total)
    return total


def to_all(value, axis):
    copies = jnp.broadcast_to(value[None], (lax.axis_size(axis), *value.shape))
    return lax.all_to_all(copies, axis, 0, 0, tiled=True)


def swapped(value, axis):
    return lax.ppermute(value, axis, [(0, 1), (1, 0)])


def shards(
    prompt, key_weight, value_weight, beta_weight, beta_bias, decay_rate, new_query, read_gain
):
    seg_len, part = prompt.shape[1], prompt.shape[2]
    heads = beta_weight.shape[1]
    tp = lax.axis_size(("x", "c"))
    sp = lax.axis_size(("zh", "zq", "y"))
    full_len = seg_len * sp
    mine = to_all(prompt[0], "x")
    other = swapped(mine, "c")
    vmem = pl.BlockSpec(memory_space=pltpu.VMEM)
    hbm = pl.BlockSpec(memory_space=pltpu.HBM)
    sides, cols = mine.shape[0], key_weight.shape[1]
    feat = tp * part
    aux = (
        jnp.pad(jnp.transpose(beta_weight).astype(F32), ((0, heads), (0, SPAN)))
        + jnp.pad(beta_bias[None], ((heads, heads - 1), (0, feat + SPAN - heads)))
        + jnp.pad(decay_rate[None], ((heads + 1, heads - 2), (0, feat + SPAN - heads)))
        + jnp.pad(new_query[0].astype(F32), ((0, heads), (feat, 0)))
    )
    key_near = key_weight.reshape(tp, part, cols)
    value_near = value_weight.reshape(tp, part, cols)
    kept = pltpu.VMEM((sides, part, cols), BF16)
    acc, beta, key_rest, query = pl.pallas_call(
        first_kernel,
        out_shape=(
            jax.ShapeDtypeStruct((seg_len, 2 * cols), F32),
            jax.ShapeDtypeStruct((seg_len, heads), F32),
            jax.ShapeDtypeStruct((sides, part, cols), BF16),
            jax.ShapeDtypeStruct((heads, SPAN), F32),
        ),
        in_specs=[vmem, vmem, hbm, hbm],
        out_specs=[vmem] * 4,
        scratch_shapes=[kept, kept, pltpu.SemaphoreType.DMA((3, sides))],
        compiler_params=pltpu.CompilerParams(vmem_limit_bytes=FIRST_MIB * 1024 * 1024),
        cost_estimate=pl.CostEstimate(
            flops=4 * seg_len * sides * part * cols, bytes_accessed=1, transcendentals=0
        ),
        name="first",
    )(mine, aux, key_near, value_near)
    span = pl.pallas_call(
        functools.partial(span_kernel, full_len),
        out_shape=jax.ShapeDtypeStruct((heads, SPAN, 2 * SPAN), BF16),
        in_specs=[vmem] * 5 + [hbm],
        out_specs=vmem,
        scratch_shapes=[
            kept,
            pltpu.SemaphoreType.DMA((sides,)),
        ],
        compiler_params=pltpu.CompilerParams(vmem_limit_bytes=SPAN_MIB * 1024 * 1024),
        cost_estimate=pl.CostEstimate(flops=10**9, bytes_accessed=1, transcendentals=0),
        name="span",
    )(other, aux, acc, beta, key_rest, value_near)
    by_head = lax.all_to_all(span, "y", 0, 0, tiled=True)
    level_y = joined(by_head).astype(BF16)
    parts = to_all(level_y, "zq")
    quads, ways = lax.axis_size("zq"), lax.axis_size("y")
    rows = SPAN // (2 * quads)
    each = rows // ways
    little = pltpu.CompilerParams(vmem_limit_bytes=4 * 1024 * 1024)
    block = jax.ShapeDtypeStruct((SPAN, SPAN), BF16)
    sent, own, level_z = pl.pallas_call(
        functools.partial(merge_kernel, quads, rows),
        out_shape=(
            block,
            jax.ShapeDtypeStruct((4 * rows, SPAN), BF16),
            jax.ShapeDtypeStruct((SPAN, 2 * SPAN), BF16),
        ),
        in_specs=[vmem] * 2,
        out_specs=[vmem] * 3,
        compiler_params=little,
        name="merge",
    )(parts, query)
    packed = pl.pallas_call(
        functools.partial(finish_kernel, quads, rows),
        out_shape=jax.ShapeDtypeStruct((ways, each + 1, SPAN), F32),
        in_specs=[vmem] * 4,
        out_specs=vmem,
        scratch_shapes=[pltpu.VMEM((SPAN, SPAN), F32)],
        compiler_params=little,
        name="finish",
    )(swapped(sent, "zh"), own, level_z, query)
    home = lax.all_to_all(packed, "y", 0, 0, tiled=True)
    return pl.pallas_call(
        last_kernel,
        out_shape=(
            jax.ShapeDtypeStruct((1, heads, each, SPAN), BF16),
            jax.ShapeDtypeStruct((1, heads, SPAN), F32),
        ),
        in_specs=[vmem] * 2,
        out_specs=[vmem] * 2,
        compiler_params=pltpu.CompilerParams(vmem_limit_bytes=4 * 1024 * 1024),
        name="last",
    )(home, read_gain[None])


def solution(mesh):
    y, x = 4, 4
    zq = 4
    zh = mesh.shape["sp"] // (zq * y)
    finer = Mesh(
        mesh.devices.reshape(mesh.shape["gr"], zh, zq, y, x, mesh.shape["tp"] // x),
        ("gr", "zh", "zq", "y", "x", "c"),
    )
    sp, tp = ("zh", "zq", "y"), ("x", "c")
    return jax.shard_map(
        shards,
        mesh=finer,
        in_specs=(
            P("gr", sp, tp),
            P(None, tp),
            P(None, tp),
            P(None, tp),
            P(tp),
            P(tp),
            P("gr", tp, None),
            P(),
        ),
        out_specs=(P("gr", tp, sp, None), P("gr", tp, None)),
        check_vma=False,
    )
```

```python
import functools

import jax
import jax.numpy as jnp
from jax import lax
from jax.experimental import pallas as pl
from jax.experimental.pallas import tpu as pltpu
from jax.sharding import Mesh
from jax.sharding import PartitionSpec as P

SPAN = 128
WIDE = 256
GROUP = 8
FIRST_MIB = 47
SPAN_MIB = 48
F32, BF16 = jnp.float32, jnp.bfloat16
NT = (((1,), (1,)), ((), ()))
NN = (((1,), (0,)), ((), ()))
TN = (((0,), (0,)), ((), ()))


def dot(a, b, dims=NN):
    return lax.dot_general(a.astype(BF16), b.astype(BF16), dims, preferred_element_type=F32)


def halves(a):
    high = a.astype(BF16)
    return high, (a - high.astype(F32)).astype(BF16)


def beta_sum(x_ref, aux_ref, side, heads):
    count, _, part = x_ref.shape
    total = None
    for j in range(count):
        start = pl.multiple_of((2 * j + side) * part, part)
        now = dot(x_ref[j], aux_ref[0:heads, pl.ds(start, part)], NT)
        total = now if total is None else total + now
    return total


def project(x_ref, weight_ref, out_ref, start):
    for n in range(0, weight_ref.shape[2], WIDE):
        total = None
        for j in range(x_ref.shape[0]):
            part = dot(x_ref[j], weight_ref[j, :, n : n + WIDE])
            total = part if total is None else total + part
        out_ref[:, start + n : start + n + WIDE] = total


def copied(src, dst, sem):
    made = pltpu.make_async_copy(src, dst, sem)
    made.start()
    return made


def first_kernel(
    x_ref, aux_ref, kw_ref, vw_ref, acc_ref, beta_ref, kw_out, query_ref, kw_own, vw_own, sems,
):
    core = lax.axis_index("c")
    sides = range(x_ref.shape[0])
    cols = kw_ref.shape[2]
    keys = [copied(kw_ref.at[2 * j + core], kw_own.at[j], sems.at[0, j]) for j in sides]
    values = [copied(vw_ref.at[2 * j + core], vw_own.at[j], sems.at[1, j]) for j in sides]
    others = [copied(kw_ref.at[2 * j + 1 - core], kw_out.at[j], sems.at[2, j]) for j in sides]
    beta_ref[...] = beta_sum(x_ref, aux_ref, core, beta_ref.shape[1])
    query = aux_ref[0 : query_ref.shape[0], kw_ref.shape[0] * kw_ref.shape[1] :]
    query_ref[...] = query * lax.rsqrt(jnp.sum(query * query, axis=-1, keepdims=True) + 1.0)
    for done in keys:
        done.wait()
    project(x_ref, kw_own, acc_ref, 0)
    for done in values:
        done.wait()
    project(x_ref, vw_own, acc_ref, cols)
    for done in others:
        done.wait()


def odd_rows(value, size):
    return jnp.concatenate(
        [value[r : r + size] for r in range(size, SPAN, 2 * size)], axis=0
    )


def woven(even, odd, size):
    parts = []
    for i in range(SPAN // (2 * size)):
        r = 2 * size * i
        parts.append(
            jnp.zeros((size, SPAN), F32) if even is None else even[r : r + size]
        )
        parts.append(odd[size * i : size * (i + 1)])
    return jnp.concatenate(parts, axis=0)


def span_kernel(
    full_len, x_ref, aux_ref, acc_ref, beta_ref, kw_ref, vw_ref, out_ref, vw_rest, sems,
):
    core = lax.axis_index("c")
    count, seg_len = x_ref.shape[:2]
    heads = out_ref.shape[0]
    cols = kw_ref.shape[2]
    rest = [
        copied(vw_ref.at[2 * j + 1 - core], vw_rest.at[j], sems.at[j]) for j in range(count)
    ]
    bias = aux_ref[heads : heads + 1, 0:heads]
    beta = beta_ref[...] + beta_sum(x_ref, aux_ref, 1 - core, heads)
    beta = jax.nn.sigmoid(beta + bias)
    keys = []
    for n in range(0, cols, WIDE):
        total = acc_ref[:, n : n + WIDE]
        for j in range(count):
            total = total + dot(x_ref[j], kw_ref[j, :, n : n + WIDE])
        keys.append(total.astype(BF16))

    row = lax.broadcasted_iota(jnp.int32, (SPAN, SPAN), 0)
    col = lax.broadcasted_iota(jnp.int32, (SPAN, SPAN), 1)
    apart = row ^ col
    lower = row > col
    eye = (row == col).astype(F32)
    place = lax.broadcasted_iota(jnp.int32, (1, SPAN), 1)
    later = (SPAN - 1 - place).astype(F32)

    jobs = [(h, s) for h in range(heads) for s in range(seg_len // SPAN)]
    per = WIDE // SPAN

    def cut(tiles, h, s):
        return tiles[h // per][s * SPAN : (s + 1) * SPAN, (h % per) * SPAN : (h % per + 1) * SPAN]

    gram = [dot(cut(keys, h, s), cut(keys, h, s), NT) for h, s in jobs]
    diag = [g * eye for g in gram]
    norm_row = [jnp.sum(d, axis=0, keepdims=True) for d in diag]
    scale_row = [lax.rsqrt(n + 1.0) for n in norm_row]
    beta_t = jnp.transpose(jnp.concatenate([beta, jnp.zeros((seg_len, SPAN - heads), F32)], axis=1))
    beta_row = [beta_t[h : h + 1, s * SPAN : (s + 1) * SPAN] for h, s in jobs]
    stack = jnp.concatenate(
        scale_row
        + [b * r for b, r in zip(beta_row, scale_row)]
        + [jnp.zeros((SPAN - 2 * len(jobs), SPAN), F32)],
        axis=0,
    )
    turned = jnp.transpose(stack)
    scale_col = [turned[:, i : i + 1] for i in range(len(jobs))]
    both_col = [turned[:, len(jobs) + i : len(jobs) + i + 1] for i in range(len(jobs))]
    low = [
        jnp.where(lower, g * b * r, 0.0) for g, b, r in zip(gram, both_col, scale_row)
    ]
    inv = [eye - jnp.where(apart == 1, lo, 0.0) for lo in low]
    log_step = [-aux_ref[heads + 1 : heads + 2, h : h + 1] / full_len for h, _ in jobs]
    val_row = [b * jnp.exp(g * later) for b, g in zip(beta_row, log_step)]
    decay = [jnp.exp(g * SPAN + jnp.zeros((1, SPAN), F32)) for g in log_step]
    key_row = [-b * r * d for b, r, d in zip(beta_row, scale_row, decay)]

    for done in rest:
        done.wait()
    pending = [(n, j) for n in range(0, cols, WIDE) for j in range(count)]
    value_acc = {n: acc_ref[:, cols + n : cols + n + WIDE] for n in range(0, cols, WIDE)}
    levels = SPAN.bit_length() - 2

    for level in range(1, levels + 1):
        size = 2**level
        inv_b = [t.astype(BF16) for t in inv]
        if size < 8:
            mask = (apart >> level) == 1
            low_m = [jnp.where(mask, lo, 0.0) for lo in low]
            mid = [dot(m, t) for m, t in zip(low_m, inv_b)]
            inv = [t - dot(tb, m) for t, tb, m in zip(inv, inv_b, mid)]
        else:
            mask = (odd_rows(apart, size) >> level) == 1
            low_m = [jnp.where(mask, odd_rows(lo, size), 0.0) for lo in low]
            mid = [woven(None, dot(m, t), size) for m, t in zip(low_m, inv_b)]
            inv = [
                woven(t, odd_rows(t, size) - dot(odd_rows(t, size), m), size)
                for t, m in zip(inv, mid)
            ]
        for _ in range(len(pending) if level == levels else 0):
            n, j = pending.pop(0)
            value_acc[n] = value_acc[n] + dot(x_ref[j], vw_rest[j, :, n : n + WIDE])
    values = [value_acc[n].astype(BF16) for n in range(0, cols, WIDE)]

    group = GROUP
    made = []
    for first in range(0, len(jobs), group):
        near = range(first, min(first + group, len(jobs)))
        split = [halves(inv[i]) for i in near]
        lows = [halves(low[i]) for i in near]
        left = [
            dot(jnp.concatenate([lo_h, lo_l], axis=1), jnp.concatenate([t_h, t_h], axis=0))
            + dot(lo_h, t_l)
            for (lo_h, lo_l), (t_h, t_l) in zip(lows, split)
        ]
        left = [((eye - inv[i]) - e).astype(BF16) for i, e in zip(near, left)]
        better = [inv[i] + dot(t_h, e) for i, (t_h, _), e in zip(near, split, left)]
        twice = [jnp.concatenate([cut(keys, *jobs[i])] * 2, axis=0) for i in near]
        x_key = [
            dot(jnp.concatenate(halves(t * key_row[i]), axis=1), k)
            for i, t, k in zip(near, better, twice)
        ]
        x_val = [
            dot(
                jnp.concatenate(halves(t * val_row[i]), axis=1),
                jnp.concatenate([cut(values, *jobs[i])] * 2, axis=0),
            )
            for i, t in zip(near, better)
        ]
        solved = [
            jnp.concatenate(
                halves(scale_col[i] * jnp.concatenate([xk, xv], axis=1)), axis=0
            )
            for i, xk, xv in zip(near, x_key, x_val)
        ]
        both = [dot(k, x, TN) for k, x in zip(twice, solved)]
        made += [
            (e[:, :SPAN] + eye * (decay[i] - 1.0), e[:, SPAN:]) for i, e in zip(near, both)
        ]

    for h in range(heads):
        total = None
        for s in range(seg_len // SPAN):
            change, write = made[h * (seg_len // SPAN) + s]
            now = jnp.concatenate([change, write], axis=1)
            total = now if total is None else now + total + dot(change, total)
        out_ref[h] = total.astype(BF16)


def rows_at(z, rows):
    return pl.ds(pl.multiple_of(z * rows, rows), rows)


def merge_kernel(quads, rows, parts_ref, query_ref, sent_ref, own_ref, level_ref):
    upper = lax.axis_index("zh") == 1
    own_z = lax.axis_index("zh") * quads + lax.axis_index("zq")
    partner_z = own_z ^ quads
    total = parts_ref[0].astype(F32)
    for j in range(1, parts_ref.shape[0]):
        now = parts_ref[j]
        total = total + now.astype(F32) + dot(now[:, :SPAN], total)
    level = total.astype(BF16)
    level_ref[...] = level
    query = jnp.broadcast_to(query_ref[pl.ds(lax.axis_index("y"), 1), :], (rows, SPAN))
    pulled = dot(query, level).astype(BF16)
    pulled = jnp.concatenate([pulled[:, :SPAN], pulled[:, SPAN:]], axis=0)

    def write(ref, z):
        picked = level_ref[rows_at(z, rows), :]
        ref[0:rows] = picked[:, :SPAN]
        ref[rows : 2 * rows] = picked[:, SPAN:]
        ref[2 * rows : 4 * rows] = pulled

    write(own_ref, own_z)

    @pl.when(upper)
    def _():
        write(sent_ref, partner_z)
        sent_ref[4 * rows :] = jnp.zeros((SPAN - 4 * rows, SPAN), BF16)

    @pl.when(jnp.logical_not(upper))
    def _():
        sent_ref[...] = level[:, SPAN:]


def finish_kernel(quads, rows, came_ref, own_ref, level_ref, query_ref, packed_ref, early_s):
    upper = lax.axis_index("zh") == 1
    own_z = lax.axis_index("zh") * quads + lax.axis_index("zq")
    came = came_ref[...].astype(F32)
    early = jnp.where(upper, came, level_ref[:, SPAN:].astype(F32))
    late = jnp.where(upper, own_ref[...].astype(F32), came[: 4 * rows])
    early_s[...] = early
    change = jnp.concatenate([late[:rows], late[2 * rows : 3 * rows]], axis=0)
    write = jnp.concatenate([late[rows : 2 * rows], late[3 * rows :]], axis=0)
    query = jnp.broadcast_to(query_ref[pl.ds(lax.axis_index("y"), 1), :], (rows, SPAN))
    high, low = halves(query)
    kept = jnp.concatenate(
        [early_s[rows_at(own_z, rows), :], dot(high, early) + dot(low, early)], axis=0
    )
    final = dot(change, early) + write + kept
    ways, each = packed_ref.shape[0], packed_ref.shape[1] - 1
    for j in range(ways):
        packed_ref[j, 0:each] = final[each * j : each * (j + 1)]
        packed_ref[j, each : each + 1] = final[rows : rows + 1]


def last_kernel(home_ref, gain_ref, state_ref, read_ref):
    each = state_ref.shape[2]
    state_ref[0] = home_ref[:, :each].astype(BF16)
    raw = home_ref[:, each]
    mean = jnp.mean(raw * raw, axis=-1, keepdims=True)
    read_ref[0] = raw * lax.rsqrt(mean + 0.05) * gain_ref[...]


def joined(parts):
    total = parts[0].astype(F32)
    for j in range(1, parts.shape[0]):
        now = parts[j]
        total = total + now.astype(F32) + dot(now[:, :SPAN], total)
    return total


def to_all(value, axis):
    copies = jnp.broadcast_to(value[None], (lax.axis_size(axis), *value.shape))
    return lax.all_to_all(copies, axis, 0, 0, tiled=True)


def swapped(value, axis):
    return lax.ppermute(value, axis, [(0, 1), (1, 0)])


def shards(
    prompt, key_weight, value_weight, beta_weight, beta_bias, decay_rate, new_query, read_gain
):
    seg_len, part = prompt.shape[1], prompt.shape[2]
    heads = beta_weight.shape[1]
    tp = lax.axis_size(("x", "c"))
    sp = lax.axis_size(("zh", "zq", "y"))
    full_len = seg_len * sp
    mine = to_all(prompt[0], "x")
    other = swapped(mine, "c")
    vmem = pl.BlockSpec(memory_space=pltpu.VMEM)
    hbm = pl.BlockSpec(memory_space=pltpu.HBM)
    sides, cols = mine.shape[0], key_weight.shape[1]
    feat = tp * part
    aux = (
        jnp.pad(jnp.transpose(beta_weight).astype(F32), ((0, heads), (0, SPAN)))
        + jnp.pad(beta_bias[None], ((heads, heads - 1), (0, feat + SPAN - heads)))
        + jnp.pad(decay_rate[None], ((heads + 1, heads - 2), (0, feat + SPAN - heads)))
        + jnp.pad(new_query[0].astype(F32), ((0, heads), (feat, 0)))
    )
    key_near = key_weight.reshape(tp, part, cols)
    value_near = value_weight.reshape(tp, part, cols)
    kept = pltpu.VMEM((sides, part, cols), BF16)
    acc, beta, key_rest, query = pl.pallas_call(
        first_kernel,
        out_shape=(
            jax.ShapeDtypeStruct((seg_len, 2 * cols), F32),
            jax.ShapeDtypeStruct((seg_len, heads), F32),
            jax.ShapeDtypeStruct((sides, part, cols), BF16),
            jax.ShapeDtypeStruct((heads, SPAN), F32),
        ),
        in_specs=[vmem, vmem, hbm, hbm],
        out_specs=[vmem] * 4,
        scratch_shapes=[kept, kept, pltpu.SemaphoreType.DMA((3, sides))],
        compiler_params=pltpu.CompilerParams(vmem_limit_bytes=FIRST_MIB * 1024 * 1024),
        cost_estimate=pl.CostEstimate(
            flops=4 * seg_len * sides * part * cols, bytes_accessed=1, transcendentals=0
        ),
        name="first",
    )(mine, aux, key_near, value_near)
    span = pl.pallas_call(
        functools.partial(span_kernel, full_len),
        out_shape=jax.ShapeDtypeStruct((heads, SPAN, 2 * SPAN), BF16),
        in_specs=[vmem] * 5 + [hbm],
        out_specs=vmem,
        scratch_shapes=[
            kept,
            pltpu.SemaphoreType.DMA((sides,)),
        ],
        compiler_params=pltpu.CompilerParams(vmem_limit_bytes=SPAN_MIB * 1024 * 1024),
        cost_estimate=pl.CostEstimate(flops=10**9, bytes_accessed=1, transcendentals=0),
        name="span",
    )(other, aux, acc, beta, key_rest, value_near)
    by_head = lax.all_to_all(span, "y", 0, 0, tiled=True)
    level_y = joined(by_head).astype(BF16)
    parts = to_all(level_y, "zq")
    quads, ways = lax.axis_size("zq"), lax.axis_size("y")
    rows = SPAN // (2 * quads)
    each = rows // ways
    little = pltpu.CompilerParams(vmem_limit_bytes=4 * 1024 * 1024)
    block = jax.ShapeDtypeStruct((SPAN, SPAN), BF16)
    sent, own, level_z = pl.pallas_call(
        functools.partial(merge_kernel, quads, rows),
        out_shape=(
            block,
            jax.ShapeDtypeStruct((4 * rows, SPAN), BF16),
            jax.ShapeDtypeStruct((SPAN, 2 * SPAN), BF16),
        ),
        in_specs=[vmem] * 2,
        out_specs=[vmem] * 3,
        compiler_params=little,
        name="merge",
    )(parts, query)
    packed = pl.pallas_call(
        functools.partial(finish_kernel, quads, rows),
        out_shape=jax.ShapeDtypeStruct((ways, each + 1, SPAN), F32),
        in_specs=[vmem] * 4,
        out_specs=vmem,
        scratch_shapes=[pltpu.VMEM((SPAN, SPAN), F32)],
        compiler_params=little,
        name="finish",
    )(swapped(sent, "zh"), own, level_z, query)
    home = lax.all_to_all(packed, "y", 0, 0, tiled=True)
    return pl.pallas_call(
        last_kernel,
        out_shape=(
            jax.ShapeDtypeStruct((1, heads, each, SPAN), BF16),
            jax.ShapeDtypeStruct((1, heads, SPAN), F32),
        ),
        in_specs=[vmem] * 2,
        out_specs=[vmem] * 2,
        compiler_params=pltpu.CompilerParams(vmem_limit_bytes=4 * 1024 * 1024),
        name="last",
    )(home, read_gain[None])


def solution(mesh):
    y, x = 4, 4
    zq = 4
    zh = mesh.shape["sp"] // (zq * y)
    finer = Mesh(
        mesh.devices.reshape(mesh.shape["gr"], zh, zq, y, x, mesh.shape["tp"] // x),
        ("gr", "zh", "zq", "y", "x", "c"),
    )
    sp, tp = ("zh", "zq", "y"), ("x", "c")
    return jax.shard_map(
        shards,
        mesh=finer,
        in_specs=(
            P("gr", sp, tp),
            P(None, tp),
            P(None, tp),
            P(None, tp),
            P(tp),
            P(tp),
            P("gr", tp, None),
            P(),
        ),
        out_specs=(P("gr", tp, sp, None), P("gr", tp, None)),
        check_vma=False,
    )
```

```python
import functools

import jax
import jax.numpy as jnp
from jax import lax
from jax.experimental import pallas as pl
from jax.experimental.pallas import tpu as pltpu
from jax.sharding import Mesh
from jax.sharding import PartitionSpec as P

SPAN = 128
WIDE = 256
GROUP = 8
FIRST_MIB = 47
SPAN_MIB = 48
F32, BF16 = jnp.float32, jnp.bfloat16
NT = (((1,), (1,)), ((), ()))
NN = (((1,), (0,)), ((), ()))
TN = (((0,), (0,)), ((), ()))


def dot(a, b, dims=NN):
    return lax.dot_general(a.astype(BF16), b.astype(BF16), dims, preferred_element_type=F32)


def halves(a):
    high = a.astype(BF16)
    return high, (a - high.astype(F32)).astype(BF16)


def beta_sum(x_ref, aux_ref, side, heads):
    count, _, part = x_ref.shape
    total = None
    for j in range(count):
        start = pl.multiple_of((2 * j + side) * part, part)
        now = dot(x_ref[j], aux_ref[0:heads, pl.ds(start, part)], NT)
        total = now if total is None else total + now
    return total


def project(x_ref, weight_ref, out_ref, start):
    for n in range(0, weight_ref.shape[2], WIDE):
        total = None
        for j in range(x_ref.shape[0]):
            part = dot(x_ref[j], weight_ref[j, :, n : n + WIDE])
            total = part if total is None else total + part
        out_ref[:, start + n : start + n + WIDE] = total


def copied(src, dst, sem):
    made = pltpu.make_async_copy(src, dst, sem)
    made.start()
    return made


def first_kernel(
    x_ref, aux_ref, kw_ref, vw_ref, acc_ref, beta_ref, kw_out, query_ref, kw_own, vw_own, sems,
):
    core = lax.axis_index("c")
    sides = range(x_ref.shape[0])
    cols = kw_ref.shape[2]
    keys = [copied(kw_ref.at[2 * j + core], kw_own.at[j], sems.at[0, j]) for j in sides]
    values = [copied(vw_ref.at[2 * j + core], vw_own.at[j], sems.at[1, j]) for j in sides]
    others = [copied(kw_ref.at[2 * j + 1 - core], kw_out.at[j], sems.at[2, j]) for j in sides]
    beta_ref[...] = beta_sum(x_ref, aux_ref, core, beta_ref.shape[1])
    query = aux_ref[0 : query_ref.shape[0], kw_ref.shape[0] * kw_ref.shape[1] :]
    query_ref[...] = query * lax.rsqrt(jnp.sum(query * query, axis=-1, keepdims=True) + 1.0)
    for done in keys:
        done.wait()
    project(x_ref, kw_own, acc_ref, 0)
    for done in values:
        done.wait()
    project(x_ref, vw_own, acc_ref, cols)
    for done in others:
        done.wait()


def odd_rows(value, size):
    return jnp.concatenate(
        [value[r : r + size] for r in range(size, SPAN, 2 * size)], axis=0
    )


def woven(even, odd, size):
    parts = []
    for i in range(SPAN // (2 * size)):
        r = 2 * size * i
        parts.append(
            jnp.zeros((size, SPAN), F32) if even is None else even[r : r + size]
        )
        parts.append(odd[size * i : size * (i + 1)])
    return jnp.concatenate(parts, axis=0)


def span_kernel(
    full_len, x_ref, aux_ref, acc_ref, beta_ref, kw_ref, vw_ref, out_ref, vw_rest, sems,
):
    core = lax.axis_index("c")
    count, seg_len = x_ref.shape[:2]
    heads = out_ref.shape[0]
    cols = kw_ref.shape[2]
    rest = [
        copied(vw_ref.at[2 * j + 1 - core], vw_rest.at[j], sems.at[j]) for j in range(count)
    ]
    bias = aux_ref[heads : heads + 1, 0:heads]
    beta = beta_ref[...] + beta_sum(x_ref, aux_ref, 1 - core, heads)
    beta = jax.nn.sigmoid(beta + bias)
    keys = []
    for n in range(0, cols, WIDE):
        total = acc_ref[:, n : n + WIDE]
        for j in range(count):
            total = total + dot(x_ref[j], kw_ref[j, :, n : n + WIDE])
        keys.append(total.astype(BF16))

    row = lax.broadcasted_iota(jnp.int32, (SPAN, SPAN), 0)
    col = lax.broadcasted_iota(jnp.int32, (SPAN, SPAN), 1)
    apart = row ^ col
    lower = row > col
    eye = (row == col).astype(F32)
    place = lax.broadcasted_iota(jnp.int32, (1, SPAN), 1)
    later = (SPAN - 1 - place).astype(F32)

    jobs = [(h, s) for h in range(heads) for s in range(seg_len // SPAN)]
    per = WIDE // SPAN

    def cut(tiles, h, s):
        return tiles[h // per][s * SPAN : (s + 1) * SPAN, (h % per) * SPAN : (h % per + 1) * SPAN]

    gram = [dot(cut(keys, h, s), cut(keys, h, s), NT) for h, s in jobs]
    diag = [g * eye for g in gram]
    norm_row = [jnp.sum(d, axis=0, keepdims=True) for d in diag]
    scale_row = [lax.rsqrt(n + 1.0) for n in norm_row]
    beta_t = jnp.transpose(jnp.concatenate([beta, jnp.zeros((seg_len, SPAN - heads), F32)], axis=1))
    beta_row = [beta_t[h : h + 1, s * SPAN : (s + 1) * SPAN] for h, s in jobs]
    stack = jnp.concatenate(
        scale_row
        + [b * r for b, r in zip(beta_row, scale_row)]
        + [jnp.zeros((SPAN - 2 * len(jobs), SPAN), F32)],
        axis=0,
    )
    turned = jnp.transpose(stack)
    scale_col = [turned[:, i : i + 1] for i in range(len(jobs))]
    both_col = [turned[:, len(jobs) + i : len(jobs) + i + 1] for i in range(len(jobs))]
    low = [
        jnp.where(lower, g * b * r, 0.0) for g, b, r in zip(gram, both_col, scale_row)
    ]
    inv = [eye - jnp.where(apart == 1, lo, 0.0) for lo in low]
    log_step = [-aux_ref[heads + 1 : heads + 2, h : h + 1] / full_len for h, _ in jobs]
    val_row = [b * jnp.exp(g * later) for b, g in zip(beta_row, log_step)]
    decay = [jnp.exp(g * SPAN + jnp.zeros((1, SPAN), F32)) for g in log_step]
    key_row = [-b * r * d for b, r, d in zip(beta_row, scale_row, decay)]

    for done in rest:
        done.wait()
    pending = [(n, j) for n in range(0, cols, WIDE) for j in range(count)]
    value_acc = {n: acc_ref[:, cols + n : cols + n + WIDE] for n in range(0, cols, WIDE)}
    levels = SPAN.bit_length() - 2

    for level in range(1, levels + 1):
        size = 2**level
        inv_b = [t.astype(BF16) for t in inv]
        if size < 8:
            mask = (apart >> level) == 1
            low_m = [jnp.where(mask, lo, 0.0) for lo in low]
            mid = [dot(m, t) for m, t in zip(low_m, inv_b)]
            inv = [t - dot(tb, m) for t, tb, m in zip(inv, inv_b, mid)]
        else:
            mask = (odd_rows(apart, size) >> level) == 1
            low_m = [jnp.where(mask, odd_rows(lo, size), 0.0) for lo in low]
            mid = [woven(None, dot(m, t), size) for m, t in zip(low_m, inv_b)]
            inv = [
                woven(t, odd_rows(t, size) - dot(odd_rows(t, size), m), size)
                for t, m in zip(inv, mid)
            ]
        for _ in range(-(-len(pending) // (levels + 1 - level))):
            n, j = pending.pop(0)
            value_acc[n] = value_acc[n] + dot(x_ref[j], vw_rest[j, :, n : n + WIDE])
    values = [value_acc[n].astype(BF16) for n in range(0, cols, WIDE)]

    group = GROUP
    made = []
    for first in range(0, len(jobs), group):
        near = range(first, min(first + group, len(jobs)))
        split = [halves(inv[i]) for i in near]
        lows = [halves(low[i]) for i in near]
        left = [
            dot(jnp.concatenate([lo_h, lo_l], axis=1), jnp.concatenate([t_h, t_h], axis=0))
            + dot(lo_h, t_l)
            for (lo_h, lo_l), (t_h, t_l) in zip(lows, split)
        ]
        left = [((eye - inv[i]) - e).astype(BF16) for i, e in zip(near, left)]
        better = [inv[i] + dot(t_h, e) for i, (t_h, _), e in zip(near, split, left)]
        twice = [jnp.concatenate([cut(keys, *jobs[i])] * 2, axis=0) for i in near]
        x_key = [
            dot(jnp.concatenate(halves(t * key_row[i]), axis=1), k)
            for i, t, k in zip(near, better, twice)
        ]
        x_val = [
            dot(
                jnp.concatenate(halves(t * val_row[i]), axis=1),
                jnp.concatenate([cut(values, *jobs[i])] * 2, axis=0),
            )
            for i, t in zip(near, better)
        ]
        solved = [
            jnp.concatenate(
                halves(scale_col[i] * jnp.concatenate([xk, xv], axis=1)), axis=0
            )
            for i, xk, xv in zip(near, x_key, x_val)
        ]
        both = [dot(k, x, TN) for k, x in zip(twice, solved)]
        made += [
            (e[:, :SPAN] + eye * (decay[i] - 1.0), e[:, SPAN:]) for i, e in zip(near, both)
        ]

    for h in range(heads):
        total = None
        for s in range(seg_len // SPAN):
            change, write = made[h * (seg_len // SPAN) + s]
            now = jnp.concatenate([change, write], axis=1)
            total = now if total is None else now + total + dot(change, total)
        out_ref[h] = total.astype(BF16)


def rows_at(z, rows):
    return pl.ds(pl.multiple_of(z * rows, rows), rows)


def merge_kernel(quads, rows, parts_ref, query_ref, sent_ref, own_ref, level_ref):
    upper = lax.axis_index("zh") == 1
    own_z = lax.axis_index("zh") * quads + lax.axis_index("zq")
    partner_z = own_z ^ quads
    both = []
    for j in range(0, parts_ref.shape[0], 2):
        before, now = parts_ref[j], parts_ref[j + 1]
        both.append(now.astype(F32) + before.astype(F32) + dot(now[:, :SPAN], before))
    total = both[1] + both[0] + dot(both[1][:, :SPAN], both[0])
    level = total.astype(BF16)
    level_ref[...] = level
    query = jnp.broadcast_to(query_ref[pl.ds(lax.axis_index("y"), 1), :], (rows, SPAN))
    pulled = dot(query, level).astype(BF16)
    pulled = jnp.concatenate([pulled[:, :SPAN], pulled[:, SPAN:]], axis=0)

    def write(ref, z):
        picked = level_ref[rows_at(z, rows), :]
        ref[0:rows] = picked[:, :SPAN]
        ref[rows : 2 * rows] = picked[:, SPAN:]
        ref[2 * rows : 4 * rows] = pulled

    write(own_ref, own_z)

    @pl.when(upper)
    def _():
        write(sent_ref, partner_z)
        sent_ref[4 * rows :] = jnp.zeros((SPAN - 4 * rows, SPAN), BF16)

    @pl.when(jnp.logical_not(upper))
    def _():
        sent_ref[...] = level[:, SPAN:]


def finish_kernel(quads, rows, came_ref, own_ref, level_ref, query_ref, packed_ref, early_s):
    upper = lax.axis_index("zh") == 1
    own_z = lax.axis_index("zh") * quads + lax.axis_index("zq")
    came = came_ref[...].astype(F32)
    early = jnp.where(upper, came, level_ref[:, SPAN:].astype(F32))
    late = jnp.where(upper, own_ref[...].astype(F32), came[: 4 * rows])
    early_s[...] = early
    change = jnp.concatenate([late[:rows], late[2 * rows : 3 * rows]], axis=0)
    write = jnp.concatenate([late[rows : 2 * rows], late[3 * rows :]], axis=0)
    query = jnp.broadcast_to(query_ref[pl.ds(lax.axis_index("y"), 1), :], (rows, SPAN))
    high, low = halves(query)
    kept = jnp.concatenate(
        [early_s[rows_at(own_z, rows), :], dot(high, early) + dot(low, early)], axis=0
    )
    final = dot(change, early) + write + kept
    ways, each = packed_ref.shape[0], packed_ref.shape[1] - 1
    for j in range(ways):
        packed_ref[j, 0:each] = final[each * j : each * (j + 1)]
        packed_ref[j, each : each + 1] = final[rows : rows + 1]


def last_kernel(home_ref, gain_ref, state_ref, read_ref):
    each = state_ref.shape[2]
    state_ref[0] = home_ref[:, :each].astype(BF16)
    raw = home_ref[:, each]
    mean = jnp.mean(raw * raw, axis=-1, keepdims=True)
    read_ref[0] = raw * lax.rsqrt(mean + 0.05) * gain_ref[...]


def joined(parts):
    pairs = parts.reshape(parts.shape[0] // 2, 2, *parts.shape[1:])
    before, now = pairs[:, 0], pairs[:, 1]
    step = jnp.einsum("bij,bjk->bik", now[:, :, :SPAN], before, preferred_element_type=F32)
    both = step + now.astype(F32) + before.astype(F32)
    return both[1] + both[0] + dot(both[1][:, :SPAN], both[0])


def to_all(value, axis):
    copies = jnp.broadcast_to(value[None], (lax.axis_size(axis), *value.shape))
    return lax.all_to_all(copies, axis, 0, 0, tiled=True)


def swapped(value, axis):
    return lax.ppermute(value, axis, [(0, 1), (1, 0)])


def shards(
    prompt, key_weight, value_weight, beta_weight, beta_bias, decay_rate, new_query, read_gain
):
    seg_len, part = prompt.shape[1], prompt.shape[2]
    heads = beta_weight.shape[1]
    tp = lax.axis_size(("x", "c"))
    sp = lax.axis_size(("zh", "zq", "y"))
    full_len = seg_len * sp
    mine = to_all(prompt[0], "x")
    other = swapped(mine, "c")
    vmem = pl.BlockSpec(memory_space=pltpu.VMEM)
    hbm = pl.BlockSpec(memory_space=pltpu.HBM)
    sides, cols = mine.shape[0], key_weight.shape[1]
    feat = tp * part
    aux = (
        jnp.pad(jnp.transpose(beta_weight).astype(F32), ((0, heads), (0, SPAN)))
        + jnp.pad(beta_bias[None], ((heads, heads - 1), (0, feat + SPAN - heads)))
        + jnp.pad(decay_rate[None], ((heads + 1, heads - 2), (0, feat + SPAN - heads)))
        + jnp.pad(new_query[0].astype(F32), ((0, heads), (feat, 0)))
    )
    key_near = key_weight.reshape(tp, part, cols)
    value_near = value_weight.reshape(tp, part, cols)
    kept = pltpu.VMEM((sides, part, cols), BF16)
    acc, beta, key_rest, query = pl.pallas_call(
        first_kernel,
        out_shape=(
            jax.ShapeDtypeStruct((seg_len, 2 * cols), F32),
            jax.ShapeDtypeStruct((seg_len, heads), F32),
            jax.ShapeDtypeStruct((sides, part, cols), BF16),
            jax.ShapeDtypeStruct((heads, SPAN), F32),
        ),
        in_specs=[vmem, vmem, hbm, hbm],
        out_specs=[vmem] * 4,
        scratch_shapes=[kept, kept, pltpu.SemaphoreType.DMA((3, sides))],
        compiler_params=pltpu.CompilerParams(vmem_limit_bytes=FIRST_MIB * 1024 * 1024),
        cost_estimate=pl.CostEstimate(
            flops=4 * seg_len * sides * part * cols, bytes_accessed=1, transcendentals=0
        ),
        name="first",
    )(mine, aux, key_near, value_near)
    span = pl.pallas_call(
        functools.partial(span_kernel, full_len),
        out_shape=jax.ShapeDtypeStruct((heads, SPAN, 2 * SPAN), BF16),
        in_specs=[vmem] * 5 + [hbm],
        out_specs=vmem,
        scratch_shapes=[
            kept,
            pltpu.SemaphoreType.DMA((sides,)),
        ],
        compiler_params=pltpu.CompilerParams(vmem_limit_bytes=SPAN_MIB * 1024 * 1024),
        cost_estimate=pl.CostEstimate(flops=10**9, bytes_accessed=1, transcendentals=0),
        name="span",
    )(other, aux, acc, beta, key_rest, value_near)
    by_head = lax.all_to_all(span, "y", 0, 0, tiled=True)
    level_y = joined(by_head).astype(BF16)
    parts = to_all(level_y, "zq")
    quads, ways = lax.axis_size("zq"), lax.axis_size("y")
    rows = SPAN // (2 * quads)
    each = rows // ways
    little = pltpu.CompilerParams(vmem_limit_bytes=4 * 1024 * 1024)
    block = jax.ShapeDtypeStruct((SPAN, SPAN), BF16)
    sent, own, level_z = pl.pallas_call(
        functools.partial(merge_kernel, quads, rows),
        out_shape=(
            block,
            jax.ShapeDtypeStruct((4 * rows, SPAN), BF16),
            jax.ShapeDtypeStruct((SPAN, 2 * SPAN), BF16),
        ),
        in_specs=[vmem] * 2,
        out_specs=[vmem] * 3,
        compiler_params=little,
        name="merge",
    )(parts, query)
    packed = pl.pallas_call(
        functools.partial(finish_kernel, quads, rows),
        out_shape=jax.ShapeDtypeStruct((ways, each + 1, SPAN), F32),
        in_specs=[vmem] * 4,
        out_specs=vmem,
        scratch_shapes=[pltpu.VMEM((SPAN, SPAN), F32)],
        compiler_params=little,
        name="finish",
    )(swapped(sent, "zh"), own, level_z, query)
    home = lax.all_to_all(packed, "y", 0, 0, tiled=True)
    return pl.pallas_call(
        last_kernel,
        out_shape=(
            jax.ShapeDtypeStruct((1, heads, each, SPAN), BF16),
            jax.ShapeDtypeStruct((1, heads, SPAN), F32),
        ),
        in_specs=[vmem] * 2,
        out_specs=[vmem] * 2,
        compiler_params=pltpu.CompilerParams(vmem_limit_bytes=4 * 1024 * 1024),
        name="last",
    )(home, read_gain[None])


def solution(mesh):
    y, x = 4, 4
    zq = 4
    zh = mesh.shape["sp"] // (zq * y)
    finer = Mesh(
        mesh.devices.reshape(mesh.shape["gr"], zh, zq, y, x, mesh.shape["tp"] // x),
        ("gr", "zh", "zq", "y", "x", "c"),
    )
    sp, tp = ("zh", "zq", "y"), ("x", "c")
    return jax.shard_map(
        shards,
        mesh=finer,
        in_specs=(
            P("gr", sp, tp),
            P(None, tp),
            P(None, tp),
            P(None, tp),
            P(tp),
            P(tp),
            P("gr", tp, None),
            P(),
        ),
        out_specs=(P("gr", tp, sp, None), P("gr", tp, None)),
        check_vma=False,
    )
```
